256 devices in a mesh: sp: 64 (over z, x, core), tp: 4 (over y).
Axes of the slice: x: 4, y: 4, z: 8, core: 2. Of those that a mesh axis runs over, the one named last changes fastest.
Arguments:
- queries: bfloat16 [40960, 2048], P('sp', 'tp'), may hold values from -164 to 164
- keys: bfloat16 [40960, 512], P('sp', 'tp'), may hold values from -6 to 6
- values: bfloat16 [40960, 512], P('sp', 'tp'), may hold values from -6 to 6
- sink: float32 [32], P('tp'), may hold values from 4 to 8
- stream: bfloat16 [40960, 2048], P(('sp', 'tp')), may hold values from -6 to 6
- out_weight: bfloat16 [2048, 2048], P('tp'), may hold values from -0.5390625 to 0.5390625
- norm_gain: float32 [2048], replicated, may hold values from 0.1 to 1.9
- gate_weight: bfloat16 [2048, 5632], P('sp', 'tp'), may hold values from -0.125 to 0.125
- up_weight: bfloat16 [2048, 5632], P('sp', 'tp'), may hold values from -0.125 to 0.125
- down_weight: bfloat16 [5632, 2048], P('tp', 'sp'), may hold values from -0.23925781 to 0.23925781
Outputs:
- result: bfloat16 [40960, 2048], P(('sp', 'tp'))
The draws below stay inside these ranges and needn't reach their ends.
All inputs are finite; a program needn't handle non-finite values.
Results may differ from the reference program's by a relative error of at most 0.019.
Values may be sent and summed in bfloat16 or wider, within the bound.
No kernel may reach another device: no remote copies, remote signals or barrier semaphores. Data moves between devices by JAX's collectives and lax.ppermute only.
A program may use at most 128 MiB of HBM per device.

```python
import jax
import jax.numpy as jnp
from jax import lax

D = 2048
HEADS = 32
KV_HEADS = 8
HEAD = 64
FF = 5632
WINDOW = 128
TOK_DEV = 640
TOKENS = 40960


def draw_queries(key, part):
    shape = (TOKENS, HEADS * HEAD)
    return jnp.clip(2.0 * jax.random.normal(key, shape, jnp.float32), -12.0, 12.0).astype(jnp.bfloat16)


def block_scale(key, shape, cuts, least, largest):
    def one(axis_at, shards_of):
        steps = jax.random.uniform(jax.random.fold_in(jax.random.fold_in(key, 6), axis_at), (shards_of,), jnp.float32, least / len(cuts), largest / len(cuts))
        return jnp.repeat(jnp.exp(steps), shape[axis_at] // shards_of).reshape((-1,) + (1,) * (len(shape) - axis_at - 1))

    gain = one(*cuts[0])
    for cut in cuts[1:]:
        gain = gain * one(*cut)
    return gain


def normal_values(own_key, extent, width, bound, cuts=(), held_as=jnp.bfloat16):
    level = block_scale(own_key, extent, cuts, -0.22, 0.18) if cuts else 1.0
    array = jax.random.normal(own_key, extent, jnp.float32) * width * level
    return jnp.minimum(jnp.maximum(array, -bound), bound).astype(held_as)


def setup_inputs(seed: int = 0) -> dict:
    key_list = jax.random.split(jax.random.key(seed), 11)
    return {
        "queries": draw_queries(jax.random.fold_in(key_list[10], 71), 0),
        "keys": normal_values(key_list[1], (TOKENS, KV_HEADS * HEAD), 1.0, 6.0, ((0, 64), (1, 4))),
        "values": normal_values(key_list[2], (TOKENS, KV_HEADS * HEAD), 1.0, 6.0, ((0, 64), (1, 4))),
        "sink": jnp.clip(4.0 + 4.0 * jax.random.uniform(key_list[3], (HEADS,), jnp.float32) ** block_scale(key_list[3], (HEADS,), ((0, 4),), -0.2, 0.2), 4.0, 8.0),
        "stream": normal_values(key_list[4], (TOKENS, D), 1.0, 6.0, ((0, 256),)),
        "out_weight": normal_values(key_list[5], (HEADS * HEAD, D), 0.09, 0.5390625, ((0, 4),)),
        "norm_gain": jnp.clip(1.0 + 0.18 * jax.random.normal(key_list[6], (D,), jnp.float32), 0.1, 1.9),
        "gate_weight": normal_values(key_list[7], (D, FF), D ** -0.5, 0.125, ((0, 64), (1, 4))),
        "up_weight": normal_values(key_list[8], (D, FF), D ** -0.5, 0.125, ((0, 64), (1, 4))),
        "down_weight": normal_values(key_list[9], (FF, D), 0.04, 0.23925781, ((0, 4), (1, 64))),
    }


def rotary(block, start):
    length = block.shape[0]
    middle = HEAD // 2
    inverse = 1.0 / 10000.0 ** (jnp.arange(0, HEAD, 2, dtype=jnp.float32) / HEAD)
    places = (start + jnp.arange(length, dtype=jnp.int32)).astype(jnp.float32)
    angles = places[:, None, None] * inverse[None, None, :]
    cosine_table = jnp.cos(angles)
    sine_table = jnp.sin(angles)
    pieces = block.astype(jnp.float32).reshape(length, -1, HEAD)
    leading = pieces[..., :middle]
    trailing = pieces[..., middle:]
    turned = jnp.concatenate([leading * cosine_table - trailing * sine_table, trailing * cosine_table + leading * sine_table], -1)
    return turned.reshape(length, -1).astype(jnp.bfloat16)

def reference(queries, keys, values, sink, stream, out_weight, norm_gain, gate_weight, up_weight, down_weight):
    length = queries.shape[0]
    blocks = length // WINDOW
    group = HEADS // KV_HEADS
    kv_width = KV_HEADS * HEAD
    turned_q = rotary(queries, 0)
    turned_k = rotary(keys, 0)
    paired = jnp.concatenate([turned_k, values], 1)
    padded = jnp.pad(paired, ((WINDOW, WINDOW), (0, 0)))
    framed = padded.reshape(blocks + 2, WINDOW, 2 * kv_width)
    banded = jnp.concatenate([framed[:-2], framed[1:-1], framed[2:]], axis=1)
    key_band = jnp.moveaxis(banded[..., :kv_width].reshape(blocks, 3 * WINDOW, KV_HEADS, HEAD), 2, 0)
    value_band = jnp.moveaxis(banded[..., kv_width:].reshape(blocks, 3 * WINDOW, KV_HEADS, HEAD), 2, 0)
    query_blocks = jnp.moveaxis(turned_q.reshape(blocks, WINDOW, KV_HEADS, group, HEAD), 2, 0)
    sink_grid = sink.reshape(KV_HEADS, group)
    query_place = jnp.arange(blocks)[:, None, None] * WINDOW + jnp.arange(WINDOW)[None, :, None]
    key_place = jnp.arange(blocks)[:, None, None] * WINDOW - WINDOW + jnp.arange(3 * WINDOW)[None, None, :]
    valid = (jnp.abs(key_place - query_place) <= WINDOW) & (key_place >= 0) & (key_place < length)

    def one_head(item):
        query_part, key_part, value_part, sink_part = item
        scores = jnp.einsum('nqgd,nsd->ngqs', query_part.astype(jnp.float32), key_part.astype(jnp.float32)) * HEAD ** (-0.5)
        scores = jnp.where(valid[:, None], scores, -jnp.inf)
        sink_here = sink_part[None, :, None]
        top = jnp.maximum(lax.optimization_barrier(jnp.max(scores, -1)), sink_here)
        raised = jnp.exp(scores - top[..., None])
        denom = lax.optimization_barrier(jnp.sum(raised, -1)) + jnp.exp(sink_here - top)
        weights = lax.optimization_barrier((raised / denom[..., None]).astype(jnp.bfloat16))
        output = jnp.einsum('ngqs,nsd->nqgd', weights.astype(jnp.float32), value_part.astype(jnp.float32))
        return output.astype(jnp.bfloat16)
    heads_out = lax.map(one_head, (query_blocks, key_band, value_band, sink_grid))
    attended = jnp.moveaxis(heads_out, 0, 2).reshape(length, HEADS * HEAD)
    mixed = (stream.astype(jnp.float32) + jnp.dot(attended, out_weight, preferred_element_type=jnp.float32)).astype(jnp.bfloat16)
    mixed_wide = mixed.astype(jnp.float32)
    scale = lax.rsqrt(lax.optimization_barrier(jnp.mean(mixed_wide * mixed_wide, -1, keepdims=True)) + 1e-06)
    normed = (mixed_wide * scale * norm_gain).astype(jnp.bfloat16)

    def feed_forward(rows):
        gate = jnp.dot(rows, gate_weight, preferred_element_type=jnp.float32)
        upward = jnp.dot(rows, up_weight, preferred_element_type=jnp.float32)
        hidden = (jax.nn.silu(gate) * upward).astype(jnp.bfloat16)
        return jnp.dot(hidden, down_weight, preferred_element_type=jnp.float32)
    lowered = lax.map(feed_forward, normed.reshape(-1, TOK_DEV, D)).reshape(length, D)
    return (mixed_wide + 0.5 * lowered).astype(jnp.bfloat16)
```

```python
import jax
import jax.numpy as jnp
from jax import lax
from jax.experimental import pallas as pl
from jax.experimental.pallas import tpu as pltpu
from jax.sharding import PartitionSpec as P


HEAD = 64
WINDOW = 128
ZN, XN, CN, YN = 8, 4, 2, 4
TILE = 128

ANY = pl.BlockSpec(memory_space=pl.ANY)
VM = pl.BlockSpec(memory_space=pltpu.VMEM)
SM = pl.BlockSpec(memory_space=pltpu.SMEM)


def x_shift(s):
    return [
        ((z * XN + x) * CN + c, (z * XN + (x + s) % XN) * CN + c)
        for z in range(ZN) for x in range(XN) for c in range(CN)
    ]


def z_shift(s):
    return [
        ((z * XN + x) * CN + c, (((z + s) % ZN) * XN + x) * CN + c)
        for z in range(ZN) for x in range(XN) for c in range(CN)
    ]


CORE_SWAP = [(i, i ^ 1) for i in range(ZN * XN * CN)]


def y_shift(s):
    return [(i, (i + s) % YN) for i in range(YN)]


def sp_move(value, pairs):
    return lax.ppermute(value, "sp", pairs)


def tp_move(value, s):
    return lax.ppermute(value, "tp", y_shift(s))


def pack_body(place, gate, up, down, k, v, mine, theirs, tail, head):
    full = gate.shape[1] // TILE // CN
    rest = CN * full * TILE
    spare = (gate.shape[1] - rest) // CN
    core = place[2]

    def put(at, low, high):
        size = low.shape[1]
        mine[:, at : at + size] = jnp.where(core == 0, low, high)
        theirs[:, at : at + size] = jnp.where(core == 0, high, low)

    at = 0
    for j in range(full):
        for value in (gate, up):
            high = (full + j) * TILE
            put(at, value[:, j * TILE : (j + 1) * TILE], value[:, high : high + TILE])
            at += TILE
    last = [value[:, rest:].astype(jnp.float32) for value in (gate, up, down)]
    other = [pltpu.roll(value, TILE // 2, 1) for value in last]
    low = lax.broadcasted_iota(jnp.int32, last[0].shape, 1) < spare
    narrow = jnp.bfloat16
    put(at, jnp.where(low, last[0], other[1]).astype(narrow), jnp.where(low, other[0], last[1]).astype(narrow))
    at += TILE
    for j in range(full):
        high = (full + j) * TILE
        put(at, down[:, j * TILE : (j + 1) * TILE], down[:, high : high + TILE])
        at += TILE
    put(at, jnp.where(low, last[2], 0.0).astype(narrow), jnp.where(low, other[2], 0.0).astype(narrow))
    tail[:, :TILE] = k[k.shape[0] - WINDOW :, :]
    tail[:, TILE:] = v[v.shape[0] - WINDOW :, :]
    head[:, :TILE] = k[:WINDOW, :]
    head[:, TILE:] = v[:WINDOW, :]


def packed(place, gate, up, down, k, v):
    depth, wide = gate.shape[0], 11 * TILE + 6 * TILE
    shard = jax.ShapeDtypeStruct((depth, wide), gate.dtype)
    halo = jax.ShapeDtypeStruct((WINDOW, 2 * TILE), k.dtype)
    return pl.pallas_call(
        pack_body,
        out_shape=(shard, shard, halo, halo),
        in_specs=[SM] + [VM] * 5,
        out_specs=(VM,) * 4,
        name="pack",
    )(place, gate, up, down.T, k, v)


class Gathering:
    def __init__(self, mine, theirs):
        self.other = sp_move(theirs, CORE_SWAP)
        near = [sp_move(mine, x_shift(s)) for s in (1, 2, 3)]
        first = jnp.concatenate([mine] + near, 0)
        half = first.shape[0] // 2
        right, left, ups, downs = first, first, [], []
        for _ in range(3):
            right = sp_move(right, z_shift(1))
            left = sp_move(left, z_shift(-1))
            ups.append(right)
            downs.append(left)
        far_up = sp_move(right[:half], z_shift(1))
        far_down = sp_move(left[half:], z_shift(-1))
        r1 = sp_move(self.other, z_shift(1))
        l1 = sp_move(self.other, z_shift(-1))
        r2 = sp_move(r1, z_shift(1))
        l2 = sp_move(l1, z_shift(-1))
        r3 = sp_move(r2, z_shift(1))
        l3 = sp_move(l2, z_shift(-1))
        opposite = sp_move(self.other, z_shift(4))
        near = jnp.concatenate([self.other, r1, l1, opposite], 0)
        far = jnp.concatenate([r2, l2, r3, l3], 0)
        nears = [near] + [sp_move(near, x_shift(s)) for s in (1, 2, 3)]
        fars = [far] + [sp_move(far, x_shift(s)) for s in (1, 2, 3)]
        self.arrays = (first, *ups, *downs, far_up, far_down, *nears, *fars)


def weight_blocks():
    found = []
    for array, back in enumerate((0, 1, 2, 3, -1, -2, -3)):
        found += [(array, s, back, s, 0) for s in range(XN)]
    found += [(7, s, 4, s, 0) for s in range(XN // 2)]
    found += [(8, s - XN // 2, 4, s, 0) for s in range(XN // 2, XN)]
    for s in range(XN):
        found += [(9 + s, i, back, s, 1) for i, back in enumerate((0, 1, -1, 4))]
        found += [(13 + s, i, back, s, 1) for i, back in enumerate((2, -2, 3, -3))]
    return found


def assemble_body(*refs):
    place, weights, (gu, dt, gu_sem, dt_sem) = refs[0], refs[1:-4], refs[-4:]
    gu_width, dt_width = gu.shape[1], dt.shape[1]
    depth = weights[0].shape[0] // XN
    z, x, c = place[0], place[1], place[2]
    for array, block, zb, xb, oc in weight_blocks():
        who = (lax.rem(z + (ZN - zb), ZN) * XN + lax.rem(x + (XN - xb), XN)) * CN
        who = who + (c if oc == 0 else 1 - c)
        spot = pl.ds(pl.multiple_of(who * depth, depth), depth)
        rows = pl.ds(block * depth, depth)
        pltpu.make_async_copy(weights[array].at[rows, pl.ds(0, gu_width)], gu.at[spot], gu_sem).start()
        pltpu.make_async_copy(
            weights[array].at[rows, pl.ds(gu_width, dt_width)], dt.at[spot], dt_sem
        ).start()
    pltpu.make_async_copy(gu, gu, gu_sem).wait()
    pltpu.make_async_copy(dt, dt, dt_sem).wait()


def assembled(place, weights):
    model = weights[0].shape[0] // XN * ZN * XN * CN
    return pl.pallas_call(
        assemble_body,
        out_shape=(
            jax.ShapeDtypeStruct((model, 11 * TILE), jnp.bfloat16),
            jax.ShapeDtypeStruct((model, 6 * TILE), jnp.bfloat16),
        ),
        in_specs=[SM] + [ANY] * len(weights),
        out_specs=(VM, VM),
        scratch_shapes=[pltpu.SemaphoreType.DMA(()), pltpu.SemaphoreType.DMA(())],
        compiler_params=pltpu.CompilerParams(vmem_limit_bytes=16 * 2**20),
        cost_estimate=pl.CostEstimate(flops=10**6, bytes_accessed=4 * model * 17 * TILE, transcendentals=0),
        name="assemble",
    )(place, *weights)


def ffn_body(xa, xb, gu, dt, out_a, out_b, x_v, h_v, sem):
    rows = xa.shape[0]
    copies = [
        pltpu.make_async_copy(ref, x_v.at[pl.ds(i * rows, rows)], sem.at[i])
        for i, ref in enumerate((xa, xb))
    ]
    for copy in copies:
        copy.start()
    for copy in copies:
        copy.wait()
    pairs = gu.shape[1] // (2 * TILE)

    def gated(j, _):
        at = pl.multiple_of(j * 2 * TILE, 2 * TILE)
        both = jnp.dot(x_v[...], gu[:, pl.ds(at, 2 * TILE)], preferred_element_type=jnp.float32)
        gate, upward = both[:, :TILE], both[:, TILE:]
        hidden = gate / (1.0 + jnp.exp(-gate)) * upward
        h_v[:, pl.ds(pl.multiple_of(j * TILE, TILE), TILE)] = hidden.astype(jnp.bfloat16)
        return 0

    lax.fori_loop(0, pairs, gated, 0)
    gate = jnp.dot(x_v[...], gu[:, pairs * 2 * TILE :], preferred_element_type=jnp.float32)
    upward = pltpu.roll(gate, TILE // 2, 1)
    hidden = gate / (1.0 + jnp.exp(-gate)) * upward
    lane = lax.broadcasted_iota(jnp.int32, hidden.shape, 1)
    hidden = jnp.where(lane < TILE // 2, hidden, 0.0)
    h_v[:, pairs * TILE :] = hidden.astype(jnp.bfloat16)

    def lowered(n, _):
        at = pl.multiple_of(n * 2 * TILE, 2 * TILE)
        part = lax.dot_general(
            h_v[...], dt[pl.ds(at, 2 * TILE), :], (((1,), (1,)), ((), ())),
            preferred_element_type=jnp.float32,
        ).astype(jnp.bfloat16)
        out_a[:, pl.ds(at, 2 * TILE)] = part[:rows]
        out_b[:, pl.ds(at, 2 * TILE)] = part[rows:]
        return 0

    lax.fori_loop(0, dt.shape[0] // (2 * TILE), lowered, 0)


def ffn(mine, partner, gu, dt):
    rows, model = mine.shape
    half = jax.ShapeDtypeStruct(mine.shape, jnp.bfloat16)
    return pl.pallas_call(
        ffn_body,
        out_shape=(half, half),
        in_specs=[ANY, ANY, VM, VM],
        out_specs=(VM, VM),
        scratch_shapes=[
            pltpu.VMEM((2 * rows, model), jnp.bfloat16),
            pltpu.VMEM((2 * rows, dt.shape[1]), jnp.bfloat16),
            pltpu.SemaphoreType.DMA((2,)),
        ],
        compiler_params=pltpu.CompilerParams(vmem_limit_bytes=24 * 2**20),
        cost_estimate=pl.CostEstimate(
            flops=4 * rows * model * (gu.shape[1] + dt.shape[1]), bytes_accessed=8 * rows * model,
            transcendentals=0,
        ),
        name="ffn",
    )(mine, partner, gu, dt)


def angle_tables(start, length):
    lane = jnp.arange(TILE, dtype=jnp.int32)
    entry = lax.rem(lane, HEAD // 2) * 2
    inverse = 1.0 / 10000.0 ** (entry.astype(jnp.float32) / HEAD)
    places = (start + jnp.arange(length, dtype=jnp.int32)).astype(jnp.float32)
    angles = places[:, None] * inverse[None, :]
    sign = jnp.where(lax.rem(lane, HEAD) < HEAD // 2, -1.0, 1.0)
    return jnp.cos(angles), jnp.sin(angles) * sign


def turned(block, cosine, sine):
    wide = block.astype(jnp.float32)
    lane = lax.broadcasted_iota(jnp.int32, wide.shape, 1)
    swapped = jnp.where(
        lax.rem(lane, HEAD) < HEAD // 2,
        pltpu.roll(wide, TILE - HEAD // 2, 1),
        pltpu.roll(wide, HEAD // 2, 1),
    )
    return (wide * cosine + swapped * sine).astype(jnp.bfloat16)


def heads_of(place, sink, q, k, v, before, after, cosine, sine, out, at_out, q_v, k_v, v_v, g):
    rows = q.shape[0]
    blocks = rows // WINDOW
    tiles = q.shape[1] // TILE * HEAD // k.shape[1]
    heads = tiles * 2
    first, last = place[4], place[5]
    lane = lax.broadcasted_iota(jnp.int32, (WINDOW, TILE), 1)
    low = lane < HEAD

    def both_halves(block):
        kept = jnp.where(low if g == 0 else ~low, block.astype(jnp.float32), 0.0)
        return (kept + pltpu.roll(kept, HEAD, 1)).astype(jnp.bfloat16)

    for n in range(blocks + 2):
        at = slice(n * WINDOW, (n + 1) * WINDOW)
        if n == 0:
            kb, vb = before[:, :TILE], before[:, TILE:]
        elif n == blocks + 1:
            kb, vb = after[:, :TILE], after[:, TILE:]
        else:
            kb, vb = k[(n - 1) * WINDOW : n * WINDOW, :], v[(n - 1) * WINDOW : n * WINDOW, :]
        k_v[at, :] = both_halves(turned(kb, cosine[at, :], sine[at, :]))
        v_v[at, :] = both_halves(vb)
    for n in range(blocks):
        angles = slice((n + 1) * WINDOW, (n + 2) * WINDOW)
        for t in range(tiles):
            lanes = slice((g * tiles + t) * TILE, (g * tiles + t + 1) * TILE)
            qt = turned(q[n * WINDOW : (n + 1) * WINDOW, lanes], cosine[angles, :], sine[angles, :])
            qt = qt * jnp.bfloat16(HEAD**-0.5)
            zero = jnp.zeros_like(qt)
            at = (n * heads + 2 * t) * WINDOW
            q_v[at : at + WINDOW, :] = jnp.where(low, qt, zero)
            q_v[at + WINDOW : at + 2 * WINDOW, :] = jnp.where(low, zero, qt)

    row = lax.broadcasted_iota(jnp.int32, (WINDOW, 3 * WINDOW), 0)
    col = lax.broadcasted_iota(jnp.int32, (WINDOW, 3 * WINDOW), 1)
    band = (col >= row) & (col - row <= 2 * WINDOW)

    def one(n, _):
        at = pl.multiple_of(n * WINDOW, WINDOW)
        floor = jnp.where((n == 0) & (first == 1), WINDOW, 0)
        ceiling = jnp.where((n == blocks - 1) & (last == 1), 2 * WINDOW, 3 * WINDOW)
        valid = band & (col >= floor) & (col < ceiling)
        qs = q_v[pl.ds(pl.multiple_of(n * heads * WINDOW, heads * WINDOW), heads * WINDOW), :]
        scores = lax.dot_general(
            qs, k_v[pl.ds(at, 3 * WINDOW), :], (((1,), (1,)), ((), ())),
            preferred_element_type=jnp.float32,
        )
        exps, denoms = [], []
        for h in range(heads):
            sunk = sink[g * heads + h]
            s = jnp.where(valid, scores[h * WINDOW : (h + 1) * WINDOW], -jnp.inf)
            top = jnp.maximum(jnp.max(s, 1, keepdims=True), sunk)
            raised = jnp.exp(s - top)
            denoms.append(jnp.sum(raised, 1, keepdims=True) + jnp.exp(sunk - top))
            exps.append(raised.astype(jnp.bfloat16))
        mixed = jnp.dot(
            jnp.concatenate(exps, 0), v_v[pl.ds(at, 3 * WINDOW), :], preferred_element_type=jnp.float32
        )
        done = [mixed[h * WINDOW : (h + 1) * WINDOW] / denoms[h] for h in range(heads)]
        for t in range(tiles):
            lanes = slice(at_out + t * TILE, at_out + (t + 1) * TILE)
            out[pl.ds(at, WINDOW), lanes] = jnp.where(low, done[2 * t], done[2 * t + 1]).astype(jnp.bfloat16)
        return 0

    lax.fori_loop(0, blocks, one, 0)


def attend_body(place, sink, q, k, v, before, after, cosine, sine, out, q_v, k_v, v_v):
    heads_of(place, sink, q, k, v, before, after, cosine, sine, out, 0, q_v, k_v, v_v, 0)


def project_body(
    place, sink, q, k, v, before, after, cosine, sine, done, weight,
    out0, out1, out2, out3, q_v, k_v, v_v, att_v, part_v, sem,
):
    rows, half = done.shape
    att_v[:, :half] = done[...]
    heads_of(place, sink, q, k, v, before, after, cosine, sine, att_v, half, q_v, k_v, v_v, 1)

    def project(n, _):
        at = pl.multiple_of(n * 2 * TILE, 2 * TILE)
        part_v[:, pl.ds(at, 2 * TILE)] = jnp.dot(
            att_v[...], weight[:, pl.ds(at, 2 * TILE)], preferred_element_type=jnp.float32
        ).astype(jnp.bfloat16)
        return 0

    lax.fori_loop(0, weight.shape[1] // (2 * TILE), project, 0)
    share = rows // YN
    copies = []
    for s, out in enumerate((out0, out1, out2, out3)):
        at = pl.multiple_of(lax.rem(place[3] + s, YN) * share, share)
        copies.append(pltpu.make_async_copy(part_v.at[pl.ds(at, share)], out, sem.at[s]))
    for copy in copies:
        copy.start()
    for copy in copies:
        copy.wait()


def attend(place, sink, q, k, v, before, after, cosine, sine, weight):
    rows, width = q.shape
    model = weight.shape[1]
    padded = rows + 2 * WINDOW
    scratch = [
        pltpu.VMEM((rows * 4, TILE), jnp.bfloat16),
        pltpu.VMEM((padded, TILE), jnp.bfloat16),
        pltpu.VMEM((padded, TILE), jnp.bfloat16),
    ]
    params = pltpu.CompilerParams(vmem_limit_bytes=40 * 2**20)
    common = (place, sink, q, k, v, before, after, cosine, sine)
    work = 16 * rows * 3 * WINDOW * TILE
    done = pl.pallas_call(
        attend_body,
        out_shape=jax.ShapeDtypeStruct((rows, width // 2), jnp.bfloat16),
        in_specs=[SM, SM] + [VM] * 7,
        out_specs=VM,
        scratch_shapes=scratch,
        compiler_params=params,
        cost_estimate=pl.CostEstimate(flops=work, bytes_accessed=4 * rows * width, transcendentals=0),
        name="attend0",
    )(*common)
    out = jax.ShapeDtypeStruct((rows // YN, model), jnp.bfloat16)
    return pl.pallas_call(
        project_body,
        out_shape=(out,) * YN,
        in_specs=[SM, SM] + [VM] * 9,
        out_specs=(ANY,) * YN,
        scratch_shapes=scratch
        + [
            pltpu.VMEM((rows, width), jnp.bfloat16),
            pltpu.VMEM((rows, model), jnp.bfloat16),
            pltpu.SemaphoreType.DMA((YN,)),
        ],
        compiler_params=params,
        cost_estimate=pl.CostEstimate(
            flops=work + 2 * rows * width * model, bytes_accessed=4 * rows * model, transcendentals=0
        ),
        name="attend1",
    )(*common, done, weight)


def layer(
    queries, keys, values, sink, stream, out_weight, norm_gain, gate_weight, up_weight, down_weight
):
    sp, tp = lax.axis_index("sp"), lax.axis_index("tp")
    rows = queries.shape[0]
    ends = ZN * XN * CN - 1
    place = jnp.stack(
        [sp // (XN * CN), lax.rem(sp // CN, XN), lax.rem(sp, CN), tp,
         (sp == 0).astype(jnp.int32), (sp == ends).astype(jnp.int32)]
    ).astype(jnp.int32)
    own, theirs, tail, head = packed(place, gate_weight, up_weight, down_weight, keys, values)
    before = sp_move(tail, [(i, i + 1) for i in range(ends)])
    after = sp_move(head, [(i + 1, i) for i in range(ends)])
    weights = Gathering(own, theirs).arrays
    cosine, sine = angle_tables(sp * rows - WINDOW, rows + 2 * WINDOW)
    parts = attend(place, sink, queries, keys, values, before, after, cosine, sine, out_weight)
    total = stream.astype(jnp.float32) + (
        parts[0].astype(jnp.float32)
        + sum(tp_move(parts[s], s).astype(jnp.float32) for s in (1, 2, 3))
    )
    mixed = total.astype(jnp.bfloat16)
    mixed_wide = mixed.astype(jnp.float32)
    scale = lax.rsqrt(jnp.mean(mixed_wide * mixed_wide, -1, keepdims=True) + 1e-06)
    normed = (mixed_wide * scale * norm_gain).astype(jnp.bfloat16)
    mine = [normed] + [tp_move(normed, s) for s in (1, 2, 3)]
    gu, dt = assembled(place, weights)
    lowered = 0.0
    for s in (2, 1, 3, 0):
        partner = sp_move(mine[s], CORE_SWAP)
        kept, sent = ffn(mine[s], partner, gu, dt)
        block = kept.astype(jnp.float32) + sp_move(sent, CORE_SWAP).astype(jnp.float32)
        if s:
            block = tp_move(block.astype(jnp.bfloat16), -s).astype(jnp.float32)
        lowered = lowered + block
    return (mixed_wide + 0.5 * lowered).astype(jnp.bfloat16)


def solution(mesh):
    placed = (
        P("sp", "tp"),
        P("sp", "tp"),
        P("sp", "tp"),
        P("tp"),
        P(("sp", "tp"), None),
        P("tp", None),
        P(),
        P("sp", "tp"),
        P("sp", "tp"),
        P("tp", "sp"),
    )
    return jax.shard_map(layer, mesh=mesh, in_specs=placed, out_specs=P(("sp", "tp"), None), check_vma=False)
```

```python
import functools

import jax
import jax.numpy as jnp
from jax import lax
from jax.experimental import pallas as pl
from jax.experimental.pallas import tpu as pltpu
from jax.sharding import PartitionSpec as P


HEAD = 64
WINDOW = 128
ZN, XN, CN, YN = 8, 4, 2, 4
TILE = 128

ANY = pl.BlockSpec(memory_space=pl.ANY)
VM = pl.BlockSpec(memory_space=pltpu.VMEM)
SM = pl.BlockSpec(memory_space=pltpu.SMEM)
HB = pl.BlockSpec(memory_space=pltpu.HBM)


def paired(at, core, step, count):
    turn = core * step if 2 * step < count else 0
    return (((at - turn + count) % count) ^ step) + turn


def x_pairs(step):
    return [
        ((z * XN + x) * CN + c, (z * XN + paired(x, c, step, XN) % XN) * CN + c)
        for z in range(ZN) for x in range(XN) for c in range(CN)
    ]


def z_pairs(step):
    return [
        ((z * XN + x) * CN + c, ((paired(z, c, step, ZN) % ZN) * XN + x) * CN + c)
        for z in range(ZN) for x in range(XN) for c in range(CN)
    ]


def x_shift(s):
    return [
        ((z * XN + x) * CN + c, (z * XN + (x + s) % XN) * CN + c)
        for z in range(ZN) for x in range(XN) for c in range(CN)
    ]


def z_shift(s):
    return [
        ((z * XN + x) * CN + c, (((z + s) % ZN) * XN + x) * CN + c)
        for z in range(ZN) for x in range(XN) for c in range(CN)
    ]


CORE_SWAP = [(i, i ^ 1) for i in range(ZN * XN * CN)]


def y_shift(s):
    return [(i, (i + s) % YN) for i in range(YN)]


def sp_move(value, pairs):
    return lax.ppermute(value, "sp", pairs)


def tp_move(value, s):
    return lax.ppermute(value, "tp", y_shift(s))


def pack_body(gate, up, down, k, v, mine, theirs, across):
    full = gate.shape[1] // TILE // CN
    rest = CN * full * TILE
    spare = (gate.shape[1] - rest) // CN
    core = sp_place()[2]

    def put(at, low, high):
        size = low.shape[1]
        mine[:, at : at + size] = jnp.where(core == 0, low, high)
        theirs[:, at : at + size] = jnp.where(core == 0, high, low)

    at = 0
    for j in range(full):
        for value in (gate, up):
            high = (full + j) * TILE
            put(at, value[:, j * TILE : (j + 1) * TILE], value[:, high : high + TILE])
            at += TILE
    last = [value[:, rest:].astype(jnp.float32) for value in (gate, up, down)]
    other = [pltpu.roll(value, TILE // 2, 1) for value in last]
    low = lax.broadcasted_iota(jnp.int32, last[0].shape, 1) < spare
    narrow = jnp.bfloat16
    put(at, jnp.where(low, last[0], other[1]).astype(narrow), jnp.where(low, other[0], last[1]).astype(narrow))
    at += TILE
    for j in range(full):
        high = (full + j) * TILE
        put(at, down[:, j * TILE : (j + 1) * TILE], down[:, high : high + TILE])
        at += TILE
    put(at, jnp.where(low, last[2], 0.0).astype(narrow), jnp.where(low, other[2], 0.0).astype(narrow))
    at += TILE
    depth = gate.shape[0]
    for lane, value in enumerate((k, v)):
        tail, head = value[value.shape[0] - WINDOW :, :], value[:WINDOW, :]
        across[:, lane * TILE : (lane + 1) * TILE] = jnp.where(core == 0, head, tail)
        kept = jnp.where(core == 0, tail, head)
        for i in range(WINDOW // depth):
            lanes = slice(at + (2 * i + lane) * TILE, at + (2 * i + lane + 1) * TILE)
            theirs[:, lanes] = kept[i * depth : (i + 1) * depth]


def packed(gate, up, down, k, v):
    depth, wide = gate.shape[0], 11 * TILE + 6 * TILE
    shard = jax.ShapeDtypeStruct((depth, wide), gate.dtype)
    wider = jax.ShapeDtypeStruct((depth, wide + WINDOW // depth * 2 * TILE), gate.dtype)
    halo = jax.ShapeDtypeStruct((WINDOW, 2 * TILE), k.dtype)
    return pl.pallas_call(
        pack_body,
        out_shape=(shard, wider, halo),
        in_specs=[VM] * 5,
        out_specs=(VM,) * 3,
        name="pack",
    )(gate, up, down.T, k, v)


def gathered_weights(mine, swapped):
    def met(value, pairs):
        return jnp.concatenate([value, sp_move(value, pairs)], 0)

    first = met(met(mine, x_pairs(2)), x_pairs(1))
    half = first.shape[0] // 2
    right, left, ups, downs = first, first, [], []
    for _ in range(3):
        right = sp_move(right, z_shift(1))
        left = sp_move(left, z_shift(-1))
        ups.append(right)
        downs.append(left)
    far_up = sp_move(right[:half], z_shift(1))
    far_down = sp_move(left[half:], z_shift(-1))
    near = met(met(swapped[:, : mine.shape[1]], z_pairs(4)), z_pairs(2))
    far = sp_move(near, z_pairs(1))
    nears = [near] + [sp_move(near, x_shift(i)) for i in (1, 2, 3)]
    fars = [far] + [sp_move(far, x_shift(i)) for i in (1, 2, 3)]
    return (first, *ups, *downs, far_up, far_down, *nears, *fars)


def weight_blocks(z, x, c):
    met = paired(x, c, 1, XN)
    xs = (x, x + 2, met, met + 2)
    found = []
    for array, back in enumerate((0, 1, 2, 3, -1, -2, -3)):
        found += [(array, i, z + ZN - back, at, c) for i, at in enumerate(xs)]
    found += [(7, i, z + 4, at, c) for i, at in enumerate(xs[:2])]
    found += [(8, i, z + 4, at, c) for i, at in enumerate(xs[2:])]
    array = 9
    for low in (z, paired(z, c, 1, ZN)):
        over = paired(low % ZN, c, 2, ZN)
        zs = (low, low + 4, over, over + 4)
        for back in range(XN):
            found += [(array, j, zz, x + XN - back, 1 - c) for j, zz in enumerate(zs)]
            array += 1
    return found


def sp_place():
    sp = lax.axis_index("sp").astype(jnp.int32)
    return sp // (XN * CN), lax.rem(sp // CN, XN), lax.rem(sp, CN)


def assemble_body(*refs, chosen, started):
    count = len(chosen)
    weights = refs[:count]
    gu, dt, gu_sem, dt_sem = refs[count + (2 if started else 0) :]
    gu_width, dt_width = gu.shape[1], dt.shape[1]
    depth = gu.shape[0] // (ZN * XN * CN)
    copies = []
    for array, block, z, x, c in weight_blocks(*sp_place()):
        if array not in chosen:
            continue
        who = (lax.rem(z, ZN) * XN + lax.rem(x, XN)) * CN + c
        spot = pl.ds(pl.multiple_of(who * depth, depth), depth)
        rows = pl.ds(block * depth, depth)
        ref = weights[chosen.index(array)]
        pltpu.make_async_copy(ref.at[rows, pl.ds(0, gu_width)], gu.at[spot], gu_sem).start()
        pltpu.make_async_copy(ref.at[rows, pl.ds(gu_width, dt_width)], dt.at[spot], dt_sem).start()
        copies.append(block)
    whole = pl.ds(0, depth * len(copies))
    pltpu.make_async_copy(gu.at[whole], gu.at[whole], gu_sem).wait()
    pltpu.make_async_copy(dt.at[whole], dt.at[whole], dt_sem).wait()


def assembled(weights, chosen, begun=()):
    model = weights[0].shape[0] // XN * ZN * XN * CN
    count = len(chosen)
    return pl.pallas_call(
        functools.partial(assemble_body, chosen=chosen, started=bool(begun)),
        out_shape=(
            jax.ShapeDtypeStruct((model, 11 * TILE), jnp.bfloat16),
            jax.ShapeDtypeStruct((model, 6 * TILE), jnp.bfloat16),
        ),
        in_specs=[ANY] * count + [VM] * len(begun),
        out_specs=(VM, VM),
        scratch_shapes=[pltpu.SemaphoreType.DMA(()), pltpu.SemaphoreType.DMA(())],
        input_output_aliases={count + i: i for i in range(len(begun))},
        compiler_params=pltpu.CompilerParams(vmem_limit_bytes=16 * 2**20),
        cost_estimate=pl.CostEstimate(flops=10**6, bytes_accessed=2 * model * 17 * TILE, transcendentals=0),
    )(*(weights[i] for i in chosen), *begun)


def ffn_body(xa, xb, gu, dt, out_a, out_b, x_v, h_v, sem):
    rows = xa.shape[0]
    copies = [
        pltpu.make_async_copy(ref, x_v.at[pl.ds(i * rows, rows)], sem.at[i])
        for i, ref in enumerate((xa, xb))
    ]
    for copy in copies:
        copy.start()
    for copy in copies:
        copy.wait()
    pairs = gu.shape[1] // (2 * TILE)
    both = jnp.dot(x_v[...], gu[...], preferred_element_type=jnp.float32)

    def tile(i):
        return both[:, i * TILE : (i + 1) * TILE]

    for j in range(pairs):
        hidden = tile(2 * j) / (1.0 + jnp.exp(-tile(2 * j))) * tile(2 * j + 1)
        h_v[:, j * TILE : (j + 1) * TILE] = hidden.astype(jnp.bfloat16)
    gate = tile(2 * pairs)
    hidden = gate / (1.0 + jnp.exp(-gate)) * pltpu.roll(gate, TILE // 2, 1)
    lane = lax.broadcasted_iota(jnp.int32, hidden.shape, 1)
    h_v[:, pairs * TILE :] = jnp.where(lane < TILE // 2, hidden, 0.0).astype(jnp.bfloat16)
    part = lax.dot_general(
        h_v[...], dt[...], (((1,), (1,)), ((), ())), preferred_element_type=jnp.float32
    ).astype(jnp.bfloat16)
    out_a[...] = part[:rows]
    out_b[...] = part[rows:]


def ffn(mine, partner, gu, dt):
    rows, model = mine.shape
    half = jax.ShapeDtypeStruct(mine.shape, jnp.bfloat16)
    return pl.pallas_call(
        ffn_body,
        out_shape=(half, half),
        in_specs=[ANY, ANY, VM, VM],
        out_specs=(VM, VM),
        scratch_shapes=[
            pltpu.VMEM((2 * rows, model), jnp.bfloat16),
            pltpu.VMEM((2 * rows, dt.shape[1]), jnp.bfloat16),
            pltpu.SemaphoreType.DMA((2,)),
        ],
        compiler_params=pltpu.CompilerParams(vmem_limit_bytes=24 * 2**20),
        cost_estimate=pl.CostEstimate(
            flops=4 * rows * model * (gu.shape[1] + dt.shape[1]), bytes_accessed=8 * rows * model,
            transcendentals=0,
        ),
        name="ffn",
    )(mine, partner, gu, dt)


def angle_tables(start, length):
    lane = jnp.arange(TILE, dtype=jnp.int32)
    entry = lax.rem(lane, HEAD // 2) * 2
    inverse = 1.0 / 10000.0 ** (entry.astype(jnp.float32) / HEAD)
    rows = length // (TILE // (HEAD // 2))
    places = (lane // (HEAD // 2))[None, :] * rows + jnp.arange(rows, dtype=jnp.int32)[:, None]
    angles = (start + places).astype(jnp.float32) * inverse[None, :]
    return jnp.cos(angles), jnp.sin(angles)


def turned(block, cosine, sine):
    wide = block.astype(jnp.float32)
    lane = lax.broadcasted_iota(jnp.int32, wide.shape, 1)
    swapped = jnp.where(
        lax.rem(lane, HEAD) < HEAD // 2,
        pltpu.roll(wide, TILE - HEAD // 2, 1),
        pltpu.roll(wide, HEAD // 2, 1),
    )
    return (wide * cosine + swapped * sine).astype(jnp.bfloat16)


def spread_angles(packed, full, sign):
    rows = packed.shape[0]
    lane = lax.broadcasted_iota(jnp.int32, packed.shape, 1)
    parts = TILE // (HEAD // 2)
    for j in range(parts):
        kept = jnp.where(lane // (HEAD // 2) == j, packed[...], 0.0)
        kept = kept + pltpu.roll(kept, HEAD // 2, 1)
        kept = kept + pltpu.roll(kept, HEAD, 1)
        if sign:
            kept = jnp.where(lax.rem(lane, HEAD) < HEAD // 2, -kept, kept)
        full[j * rows : (j + 1) * rows, :] = kept


def spread_keys(k, v, swapped, across, cosine, sine, k_v, v_v):
    rows = k.shape[0]
    low = lax.broadcasted_iota(jnp.int32, (WINDOW, TILE), 1) < HEAD

    def both_halves(block, g):
        kept = jnp.where(low if g == 0 else ~low, block.astype(jnp.float32), 0.0)
        return (kept + pltpu.roll(kept, HEAD, 1)).astype(jnp.bfloat16)

    blocks = rows // WINDOW
    core = sp_place()[2]
    parts = WINDOW // swapped.shape[0]
    start = swapped.shape[1] - parts * 2 * TILE
    inside = []
    for lane in range(2):
        spots = [start + (2 * i + lane) * TILE for i in range(parts)]
        inside.append(jnp.concatenate([swapped[:, at : at + TILE] for at in spots], 0))
    outside = [across[:, :TILE], across[:, TILE:]]
    for n in range(blocks + 2):
        at = slice(n * WINDOW, (n + 1) * WINDOW)
        if n == 0:
            kb, vb = (jnp.where(core == 0, a, b) for a, b in zip(outside, inside))
        elif n == blocks + 1:
            kb, vb = (jnp.where(core == 0, b, a) for a, b in zip(outside, inside))
        else:
            kb, vb = k[(n - 1) * WINDOW : n * WINDOW, :], v[(n - 1) * WINDOW : n * WINDOW, :]
        kb = turned(kb, cosine[at, :], sine[at, :])
        for g in range(2):
            k_v[g, at, :] = both_halves(kb, g)
            v_v[g, at, :] = both_halves(vb, g)
    spare = k_v.shape[1] - rows - 2 * WINDOW
    for g in range(2):
        k_v[g, rows + 2 * WINDOW :, :] = jnp.zeros((spare, TILE), jnp.bfloat16)
        v_v[g, rows + 2 * WINDOW :, :] = jnp.zeros((spare, TILE), jnp.bfloat16)


def attend_shares(shares, sink, q, cosine, sine, k_v, v_v, copy, weight, outs, q_v, att_v):
    rows = q.shape[0]
    share = rows // YN
    step = share // 2
    tiles = q.shape[1] // TILE
    heads = 4
    sp, tp = lax.axis_index("sp").astype(jnp.int32), lax.axis_index("tp").astype(jnp.int32)
    floor = jnp.where(sp == 0, WINDOW, 0)
    ceiling = jnp.where(sp == ZN * XN * CN - 1, rows + WINDOW, rows + 2 * WINDOW)
    low = lax.broadcasted_iota(jnp.int32, (step, TILE), 1) < HEAD
    row = lax.broadcasted_iota(jnp.int32, (step, 3 * WINDOW), 0)
    col = lax.broadcasted_iota(jnp.int32, (step, 3 * WINDOW), 1)
    band = (col >= row) & (col - row <= 2 * WINDOW)

    def one(i, _):
        ahead = jnp.where(i < 2, shares[0], shares[1])
        base = pl.multiple_of(lax.rem(tp + ahead, YN) * share + lax.rem(i, 2) * step, 16)
        to = pl.multiple_of(i * step, 16)
        valid = band & (col >= floor - base) & (col < ceiling - base)
        angles = pl.ds(pl.multiple_of(base + WINDOW, 16), step)
        cos_here, sin_here = cosine[angles, :], sine[angles, :]
        for t in range(tiles):
            qt = turned(q[pl.ds(base, step), t * TILE : (t + 1) * TILE], cos_here, sin_here)
            qt = qt * jnp.bfloat16(HEAD**-0.5)
            zero = jnp.zeros_like(qt)
            q_v[2 * t * step : (2 * t + 1) * step, :] = jnp.where(low, qt, zero)
            q_v[(2 * t + 1) * step : (2 * t + 2) * step, :] = jnp.where(low, zero, qt)
        for g in range(2):
            scores = lax.dot_general(
                q_v[g * heads * step : (g + 1) * heads * step, :],
                k_v[g, pl.ds(base, 3 * WINDOW), :],
                (((1,), (1,)), ((), ())),
                preferred_element_type=jnp.float32,
            )
            exps, denoms = [], []
            for h in range(heads):
                sunk = sink[g * heads + h]
                s = jnp.where(valid, scores[h * step : (h + 1) * step], -jnp.inf)
                top = jnp.maximum(jnp.max(s, 1, keepdims=True), sunk)
                raised = jnp.exp(s - top)
                denoms.append(jnp.sum(raised, 1, keepdims=True) + jnp.exp(sunk - top))
                exps.append(raised.astype(jnp.bfloat16))
            mixed = jnp.dot(
                jnp.concatenate(exps, 0), v_v[g, pl.ds(base, 3 * WINDOW), :],
                preferred_element_type=jnp.float32,
            )
            done = [mixed[h * step : (h + 1) * step] / denoms[h] for h in range(heads)]
            for t in range(2):
                lanes = slice((2 * g + t) * TILE, (2 * g + t + 1) * TILE)
                att_v[pl.ds(to, step), lanes] = jnp.where(low, done[2 * t], done[2 * t + 1]).astype(jnp.bfloat16)
        return 0

    lax.fori_loop(0, 4, one, 0)
    copy.wait()

    def project(n, _):
        at = pl.multiple_of(n * 2 * TILE, 2 * TILE)
        part = jnp.dot(
            att_v[...], weight[:, pl.ds(at, 2 * TILE)], preferred_element_type=jnp.float32
        ).astype(jnp.bfloat16)
        for i, out in enumerate(outs):
            out[:, pl.ds(at, 2 * TILE)] = part[i * share : (i + 1) * share]
        return 0

    lax.fori_loop(0, weight.shape[1] // (2 * TILE), project, 0)


def first_body(
    sink, q, k, v, swapped, across, cosine, sine, weight,
    out1, out3, k_v, v_v, q_v, att_v, cos_v, sin_v, w_v, sem,
):
    copy = pltpu.make_async_copy(weight, w_v, sem)
    copy.start()
    spread_angles(cosine, cos_v, False)
    spread_angles(sine, sin_v, True)
    spread_keys(k, v, swapped, across, cos_v, sin_v, k_v, v_v)
    attend_shares((1, 3), sink, q, cos_v, sin_v, k_v, v_v, copy, w_v, (out1, out3), q_v, att_v)


def second_body(
    sink, q, cosine, sine, k_v, v_v, weight, out2, out0, q_v, att_v, cos_v, sin_v, w_v, sem
):
    copy = pltpu.make_async_copy(weight, w_v, sem)
    copy.start()
    spread_angles(cosine, cos_v, False)
    spread_angles(sine, sin_v, True)
    attend_shares((2, 0), sink, q, cos_v, sin_v, k_v, v_v, copy, w_v, (out2, out0), q_v, att_v)


def attend(sink, q, k, v, swapped, across, cosine, sine, weight):
    rows, width = q.shape
    model = weight.shape[1]
    step = rows // YN // 2
    part = jax.ShapeDtypeStruct((rows // YN, model), jnp.bfloat16)
    spread = jax.ShapeDtypeStruct((2, rows + 3 * WINDOW - step, TILE), jnp.bfloat16)
    scratch = [
        pltpu.VMEM((8 * step, TILE), jnp.bfloat16),
        pltpu.VMEM((rows // 2, width), jnp.bfloat16),
        pltpu.VMEM((rows + 2 * WINDOW, TILE), jnp.float32),
        pltpu.VMEM((rows + 2 * WINDOW, TILE), jnp.float32),
        pltpu.VMEM((width, model), jnp.bfloat16),
        pltpu.SemaphoreType.DMA(()),
    ]
    params = pltpu.CompilerParams(vmem_limit_bytes=32 * 2**20)
    cost = pl.CostEstimate(flops=rows * width * model * 3, bytes_accessed=4 * rows * model, transcendentals=0)
    one, three, keys, values = pl.pallas_call(
        first_body,
        out_shape=(part, part, spread, spread),
        in_specs=[SM] + [VM] * 7 + [HB],
        out_specs=(VM,) * 4,
        scratch_shapes=scratch,
        compiler_params=params,
        cost_estimate=cost,
        name="attend0",
    )(sink, q, k, v, swapped, across, cosine, sine, weight)
    two, zero = pl.pallas_call(
        second_body,
        out_shape=(part, part),
        in_specs=[SM] + [VM] * 5 + [HB],
        out_specs=(VM,) * 2,
        scratch_shapes=scratch,
        compiler_params=params,
        cost_estimate=cost,
        name="attend1",
    )(sink, q, cosine, sine, keys, values, weight)
    return zero, one, two, three


def layer(
    queries, keys, values, sink, stream, out_weight, norm_gain, gate_weight, up_weight, down_weight
):
    sp = lax.axis_index("sp")
    rows = queries.shape[0]
    ends = ZN * XN * CN - 1
    own, theirs, across = packed(gate_weight, up_weight, down_weight, keys, values)
    chips = [(i, i + 1) for i in range(1, ends, CN)]
    across = sp_move(across, chips + [(b, a) for a, b in chips])
    swapped = sp_move(theirs, CORE_SWAP)
    weights = gathered_weights(own, swapped)
    cosine, sine = angle_tables(sp * rows - WINDOW, rows + 2 * WINDOW)
    parts = attend(sink, queries, keys, values, swapped, across, cosine, sine, out_weight)
    total = stream.astype(jnp.float32) + (
        parts[0].astype(jnp.float32)
        + sum(tp_move(parts[s], s).astype(jnp.float32) for s in (1, 2, 3))
    )
    mixed = total.astype(jnp.bfloat16)
    mixed_wide = mixed.astype(jnp.float32)
    scale = lax.rsqrt(jnp.mean(mixed_wide * mixed_wide, -1, keepdims=True) + 1e-06)
    normed = (mixed_wide * scale * norm_gain).astype(jnp.bfloat16)
    mine = [normed] + [tp_move(normed, s) for s in (1, 2, 3)]
    late = (7, 8, 14, 15, 16)
    early = tuple(i for i in range(len(weights)) if i not in late)
    gu, dt = assembled(weights, late, assembled(weights, early))
    lowered = 0.0
    for s in (2, 1, 3, 0):
        partner = sp_move(mine[s], CORE_SWAP)
        kept, sent = ffn(mine[s], partner, gu, dt)
        block = kept.astype(jnp.float32) + sp_move(sent, CORE_SWAP).astype(jnp.float32)
        if s:
            block = tp_move(block.astype(jnp.bfloat16), -s).astype(jnp.float32)
        lowered = lowered + block
    return (mixed_wide + 0.5 * lowered).astype(jnp.bfloat16)


def solution(mesh):
    placed = (
        P("sp", "tp"),
        P("sp", "tp"),
        P("sp", "tp"),
        P("tp"),
        P(("sp", "tp"), None),
        P("tp", None),
        P(),
        P("sp", "tp"),
        P("sp", "tp"),
        P("tp", "sp"),
    )
    return jax.shard_map(
        layer, mesh=mesh, in_specs=placed, out_specs=P(("sp", "tp"), None), check_vma=False
    )
```

```python
import functools

import jax
import jax.numpy as jnp
from jax import lax
from jax.experimental import pallas as pl
from jax.experimental.pallas import tpu as pltpu
from jax.sharding import PartitionSpec as P


HEAD = 64
WINDOW = 128
ZN, XN, CN, YN = 8, 4, 2, 4
TILE = 128

ANY = pl.BlockSpec(memory_space=pl.ANY)
VM = pl.BlockSpec(memory_space=pltpu.VMEM)
SM = pl.BlockSpec(memory_space=pltpu.SMEM)
HB = pl.BlockSpec(memory_space=pltpu.HBM)


def paired(at, core, step, count):
    turn = core * step if 2 * step < count else 0
    return (((at - turn + count) % count) ^ step) + turn


def z_pairs(step):
    return [
        ((z * XN + x) * CN + c, ((paired(z, c, step, ZN) % ZN) * XN + x) * CN + c)
        for z in range(ZN) for x in range(XN) for c in range(CN)
    ]


def x_pairs(step):
    return [
        ((z * XN + x) * CN + c, (z * XN + paired(x, c, step, XN) % XN) * CN + c)
        for z in range(ZN) for x in range(XN) for c in range(CN)
    ]


def x_shift(s):
    return [
        ((z * XN + x) * CN + c, (z * XN + (x + s) % XN) * CN + c)
        for z in range(ZN) for x in range(XN) for c in range(CN)
    ]


def z_shift(s):
    return [
        ((z * XN + x) * CN + c, (((z + s) % ZN) * XN + x) * CN + c)
        for z in range(ZN) for x in range(XN) for c in range(CN)
    ]


def z_apart():
    return [
        ((z * XN + x) * CN + c, (((z + 1 - 2 * c) % ZN) * XN + x) * CN + c)
        for z in range(ZN) for x in range(XN) for c in range(CN)
    ]


def x_apart():
    return [
        ((z * XN + x) * CN + c, (z * XN + (x + 1 - 2 * c) % XN) * CN + c)
        for z in range(ZN) for x in range(XN) for c in range(CN)
    ]


def y_apart():
    return [
        (((p * CN + c) * YN + y), (p * CN + c) * YN + (y + 1 - 2 * c) % YN)
        for p in range(ZN * XN) for c in range(CN) for y in range(YN)
    ]


CORE_SWAP = [(i, i ^ 1) for i in range(ZN * XN * CN)]


def y_shift(s):
    return [(i, (i + s) % YN) for i in range(YN)]


def sp_move(value, pairs):
    return lax.ppermute(value, "sp", pairs)


def tp_move(value, s):
    return lax.ppermute(value, "tp", y_shift(s))


def pack_body(gate, up, down, k, v, mine, theirs, across):
    full = gate.shape[1] // TILE // CN
    rest = CN * full * TILE
    spare = (gate.shape[1] - rest) // CN
    core = sp_place()[2]

    def put(at, low, high):
        size = low.shape[1]
        mine[:, at : at + size] = jnp.where(core == 0, low, high)
        theirs[:, at : at + size] = jnp.where(core == 0, high, low)

    at = 0
    for j in range(full):
        for value in (gate, up):
            high = (full + j) * TILE
            put(at, value[:, j * TILE : (j + 1) * TILE], value[:, high : high + TILE])
            at += TILE
    last = [value[:, rest:].astype(jnp.float32) for value in (gate, up, down)]
    other = [pltpu.roll(value, TILE // 2, 1) for value in last]
    low = lax.broadcasted_iota(jnp.int32, last[0].shape, 1) < spare
    narrow = jnp.bfloat16
    put(at, jnp.where(low, last[0], other[1]).astype(narrow), jnp.where(low, other[0], last[1]).astype(narrow))
    at += TILE
    for j in range(full):
        high = (full + j) * TILE
        put(at, down[:, j * TILE : (j + 1) * TILE], down[:, high : high + TILE])
        at += TILE
    put(at, jnp.where(low, last[2], 0.0).astype(narrow), jnp.where(low, other[2], 0.0).astype(narrow))
    at += TILE
    depth = gate.shape[0]
    for lane, value in enumerate((k, v)):
        tail, head = value[value.shape[0] - WINDOW :, :], value[:WINDOW, :]
        across[:, lane * TILE : (lane + 1) * TILE] = jnp.where(core == 0, head, tail)
        kept = jnp.where(core == 0, tail, head)
        for i in range(WINDOW // depth):
            lanes = slice(at + (2 * i + lane) * TILE, at + (2 * i + lane + 1) * TILE)
            theirs[:, lanes] = kept[i * depth : (i + 1) * depth]


def packed(gate, up, down, k, v):
    depth, wide = gate.shape[0], 11 * TILE + 6 * TILE
    shard = jax.ShapeDtypeStruct((depth, wide), gate.dtype)
    wider = jax.ShapeDtypeStruct((depth, wide + WINDOW // depth * 2 * TILE), gate.dtype)
    halo = jax.ShapeDtypeStruct((WINDOW, 2 * TILE), k.dtype)
    return pl.pallas_call(
        pack_body,
        out_shape=(shard, wider, halo),
        in_specs=[VM] * 5,
        out_specs=(VM,) * 3,
        name="pack",
    )(gate, up, down.T, k, v)


def gathered_weights(mine, swapped):
    def met(value, pairs):
        return jnp.concatenate([value, sp_move(value, pairs)], 0)

    first = jnp.concatenate([mine] + [sp_move(mine, x_shift(i)) for i in (1, 2, 3)], 0)
    right, left, ups, downs = first, first, [], []
    for _ in range(3):
        right = sp_move(right, z_shift(1))
        left = sp_move(left, z_shift(-1))
        ups.append(right)
        downs.append(left)
    opposite = jnp.where(sp_place()[2] == 0, right, left)
    apart = sp_move(opposite, z_apart())
    near = met(met(swapped[:, : mine.shape[1]], z_pairs(4)), z_pairs(2))
    far = sp_move(near, z_pairs(1))
    nears = [met(near, x_pairs(2))]
    nears.append(sp_move(nears[0], x_pairs(1)))
    fars = [far] + [sp_move(far, x_shift(i)) for i in (1, 3)]
    fars.append(sp_move(jnp.where(sp_place()[2] == 0, *fars[1:]), x_apart()))
    return (first, *ups, *downs, apart, *nears, *fars)


def weight_blocks(z, x, c):
    xs = [x + XN - back for back in range(XN)]
    found = []
    for array, back in enumerate((0, 1, 2, 3, -1, -2, -3)):
        found += [(array, i, z + ZN - back, at, c) for i, at in enumerate(xs)]
    found += [(7, i, z + 4, at, c) for i, at in enumerate(xs)]
    array = 8
    for low in (z, paired(z, c, 1, ZN)):
        over = paired(low % ZN, c, 2, ZN)
        zs = (low, low + 4, over, over + 4)
        if array == 8:
            met = paired(x, c, 1, XN)
            groups = ((x, x + 2), (met, met + 2))
        else:
            groups = ((xs[0],), (xs[1],), (xs[3],), (xs[2],))
        for group in groups:
            found += [(array, i * len(zs) + j, zz, at, 1 - c) for i, at in enumerate(group) for j, zz in enumerate(zs)]
            array += 1
    return found


def sp_place():
    sp = lax.axis_index("sp").astype(jnp.int32)
    return sp // (XN * CN), lax.rem(sp // CN, XN), lax.rem(sp, CN)


def assemble_body(*refs, chosen, started):
    count = len(chosen)
    weights = refs[:count]
    gu, dt, gu_sem, dt_sem = refs[count + (2 if started else 0) :]
    gu_width, dt_width = gu.shape[1], dt.shape[1]
    depth = gu.shape[0] // (ZN * XN * CN)
    copies = []
    for array, block, z, x, c in weight_blocks(*sp_place()):
        if array not in chosen:
            continue
        who = (lax.rem(z, ZN) * XN + lax.rem(x, XN)) * CN + c
        spot = pl.ds(pl.multiple_of(who * depth, depth), depth)
        rows = pl.ds(block * depth, depth)
        ref = weights[chosen.index(array)]
        pltpu.make_async_copy(ref.at[rows, pl.ds(0, gu_width)], gu.at[spot], gu_sem).start()
        pltpu.make_async_copy(ref.at[rows, pl.ds(gu_width, dt_width)], dt.at[spot], dt_sem).start()
        copies.append(block)
    whole = pl.ds(0, depth * len(copies))
    pltpu.make_async_copy(gu.at[whole], gu.at[whole], gu_sem).wait()
    pltpu.make_async_copy(dt.at[whole], dt.at[whole], dt_sem).wait()


def assembled(weights, chosen, begun=()):
    model = weights[0].shape[0] // XN * ZN * XN * CN
    count = len(chosen)
    return pl.pallas_call(
        functools.partial(assemble_body, chosen=chosen, started=bool(begun)),
        out_shape=(
            jax.ShapeDtypeStruct((model, 11 * TILE), jnp.bfloat16),
            jax.ShapeDtypeStruct((model, 6 * TILE), jnp.bfloat16),
        ),
        in_specs=[ANY] * count + [VM] * len(begun),
        out_specs=(VM, VM),
        scratch_shapes=[pltpu.SemaphoreType.DMA(()), pltpu.SemaphoreType.DMA(())],
        input_output_aliases={count + i: i for i in range(len(begun))},
        compiler_params=pltpu.CompilerParams(vmem_limit_bytes=16 * 2**20),
        cost_estimate=pl.CostEstimate(flops=10**6, bytes_accessed=2 * model * 17 * TILE, transcendentals=0),
    )(*(weights[i] for i in chosen), *begun)


def ffn_body(*refs, starts, looped):
    xs, (gu, dt, kept, sent, x_v, h_v, sem) = refs[:-7], refs[-7:]
    rows = x_v.shape[0] // len(xs)
    copies = [
        pltpu.make_async_copy(ref.at[pl.ds(start, rows)], x_v.at[pl.ds(i * rows, rows)], sem.at[i])
        for i, (ref, start) in enumerate(zip(xs, starts))
    ]
    for copy in copies:
        copy.start()
    for copy in copies:
        copy.wait()
    pairs = gu.shape[1] // (2 * TILE)
    some = kept.shape[0]

    def activated(gate, upward):
        return gate / (1.0 + jnp.exp(-gate)) * upward

    if not looped:
        both = jnp.dot(x_v[...], gu[...], preferred_element_type=jnp.float32)
        for j in range(pairs):
            gate, upward = (both[:, i * TILE : (i + 1) * TILE] for i in (2 * j, 2 * j + 1))
            h_v[:, j * TILE : (j + 1) * TILE] = activated(gate, upward).astype(jnp.bfloat16)
        gate = both[:, pairs * 2 * TILE :]
    else:

        def gated(j, _):
            at = pl.multiple_of(j * 2 * TILE, 2 * TILE)
            both = jnp.dot(x_v[...], gu[:, pl.ds(at, 2 * TILE)], preferred_element_type=jnp.float32)
            hidden = activated(both[:, :TILE], both[:, TILE:])
            h_v[:, pl.ds(pl.multiple_of(j * TILE, TILE), TILE)] = hidden.astype(jnp.bfloat16)
            return 0

        lax.fori_loop(0, pairs, gated, 0)
        gate = jnp.dot(x_v[...], gu[:, pairs * 2 * TILE :], preferred_element_type=jnp.float32)
    hidden = activated(gate, pltpu.roll(gate, TILE // 2, 1))
    lane = lax.broadcasted_iota(jnp.int32, hidden.shape, 1)
    h_v[:, pairs * TILE :] = jnp.where(lane < TILE // 2, hidden, 0.0).astype(jnp.bfloat16)
    width = 4 * TILE

    def lowered(n, _):
        at = pl.multiple_of(n * width, width)
        part = lax.dot_general(
            h_v[...], dt[pl.ds(at, width), :], (((1,), (1,)), ((), ())), preferred_element_type=jnp.float32
        ).astype(jnp.bfloat16)
        kept[:, pl.ds(at, width)] = part[:some]
        sent[:, pl.ds(at, width)] = part[some:]
        return 0

    lax.fori_loop(0, dt.shape[0] // width, lowered, 0)


def ffn(share, pieces, gu, dt, looped):
    model = pieces[0][0].shape[1]
    rows = share * len(pieces)
    half = jax.ShapeDtypeStruct((rows // 2, model), jnp.bfloat16)
    return pl.pallas_call(
        functools.partial(ffn_body, starts=tuple(start for _, start in pieces), looped=looped),
        out_shape=(half, half),
        in_specs=[ANY] * len(pieces) + [VM, VM],
        out_specs=(VM, VM),
        scratch_shapes=[
            pltpu.VMEM((rows, model), jnp.bfloat16),
            pltpu.VMEM((rows, dt.shape[1]), jnp.bfloat16),
            pltpu.SemaphoreType.DMA((len(pieces),)),
        ],
        compiler_params=pltpu.CompilerParams(vmem_limit_bytes=24 * 2**20),
        cost_estimate=pl.CostEstimate(
            flops=2 * rows * model * (gu.shape[1] + dt.shape[1]), bytes_accessed=4 * rows * model,
            transcendentals=0,
        ),
        name="ffn",
    )(*(array for array, _ in pieces), gu, dt)


def angle_tables(start, length):
    lane = jnp.arange(TILE, dtype=jnp.int32)
    entry = lax.rem(lane, HEAD // 2) * 2
    inverse = 1.0 / 10000.0 ** (entry.astype(jnp.float32) / HEAD)
    rows = length // (TILE // (HEAD // 2))
    places = (lane // (HEAD // 2))[None, :] * rows + jnp.arange(rows, dtype=jnp.int32)[:, None]
    angles = (start + places).astype(jnp.float32) * inverse[None, :]
    return jnp.cos(angles), jnp.sin(angles)


def turned(block, cosine, sine):
    wide = block.astype(jnp.float32)
    lane = lax.broadcasted_iota(jnp.int32, wide.shape, 1)
    swapped = jnp.where(
        lax.rem(lane, HEAD) < HEAD // 2,
        pltpu.roll(wide, TILE - HEAD // 2, 1),
        pltpu.roll(wide, HEAD // 2, 1),
    )
    return (wide * cosine + swapped * sine).astype(jnp.bfloat16)


def spread_angles(packed, full, sign):
    rows = packed.shape[0]
    lane = lax.broadcasted_iota(jnp.int32, packed.shape, 1)
    parts = TILE // (HEAD // 2)
    for j in range(parts):
        kept = jnp.where(lane // (HEAD // 2) == j, packed[...], 0.0)
        kept = kept + pltpu.roll(kept, HEAD // 2, 1)
        kept = kept + pltpu.roll(kept, HEAD, 1)
        if sign:
            kept = jnp.where(lax.rem(lane, HEAD) < HEAD // 2, -kept, kept)
        full[j * rows : (j + 1) * rows, :] = kept


def spread_keys(k, v, swapped, across, cosine, sine, k_v, v_v):
    rows = k.shape[0]
    low = lax.broadcasted_iota(jnp.int32, (WINDOW, TILE), 1) < HEAD

    def both_halves(block, g):
        kept = jnp.where(low if g == 0 else ~low, block.astype(jnp.float32), 0.0)
        return (kept + pltpu.roll(kept, HEAD, 1)).astype(jnp.bfloat16)

    blocks = rows // WINDOW
    core = sp_place()[2]
    parts = WINDOW // swapped.shape[0]
    start = swapped.shape[1] - parts * 2 * TILE
    inside = []
    for lane in range(2):
        spots = [start + (2 * i + lane) * TILE for i in range(parts)]
        inside.append(jnp.concatenate([swapped[:, at : at + TILE] for at in spots], 0))
    outside = [across[:, :TILE], across[:, TILE:]]

    def put(at, kb, vb):
        kb = turned(kb, cosine[at, :], sine[at, :])
        for g in range(2):
            k_v[g, at, :] = both_halves(kb, g)
            v_v[g, at, :] = both_halves(vb, g)

    put(slice(0, WINDOW), *(jnp.where(core == 0, a, b) for a, b in zip(outside, inside)))
    for n in range(blocks):
        at = slice(n * WINDOW, (n + 1) * WINDOW)
        put(slice((n + 1) * WINDOW, (n + 2) * WINDOW), k[at, :], v[at, :])
    ends = slice(rows + WINDOW, rows + 2 * WINDOW)
    put(ends, *(jnp.where(core == 0, b, a) for a, b in zip(outside, inside)))
    spare = k_v.shape[1] - rows - 2 * WINDOW
    for g in range(2):
        k_v[g, rows + 2 * WINDOW :, :] = jnp.zeros((spare, TILE), jnp.bfloat16)
        v_v[g, rows + 2 * WINDOW :, :] = jnp.zeros((spare, TILE), jnp.bfloat16)


def attend_shares(shares, sink, q, cosine, sine, k_v, v_v, copy, weight, outs, q_v, att_v):
    rows = q.shape[0]
    share = rows // YN
    step = share // 2
    tiles = q.shape[1] // TILE
    heads = 4
    sp, tp = lax.axis_index("sp").astype(jnp.int32), lax.axis_index("tp").astype(jnp.int32)
    floor = jnp.where(sp == 0, WINDOW, 0)
    ceiling = jnp.where(sp == ZN * XN * CN - 1, rows + WINDOW, rows + 2 * WINDOW)
    low = lax.broadcasted_iota(jnp.int32, (step, TILE), 1) < HEAD
    row = lax.broadcasted_iota(jnp.int32, (step, 3 * WINDOW), 0)
    col = lax.broadcasted_iota(jnp.int32, (step, 3 * WINDOW), 1)
    band = (col >= row) & (col - row <= 2 * WINDOW)

    def one(i, _):
        ahead = jnp.where(i < 2, shares[0], shares[1])
        base = pl.multiple_of(lax.rem(tp + ahead, YN) * share + lax.rem(i, 2) * step, 16)
        to = pl.multiple_of(i * step, 16)
        valid = band & (col >= floor - base) & (col < ceiling - base)
        angles = pl.ds(pl.multiple_of(base + WINDOW, 16), step)
        cos_here, sin_here = cosine[angles, :], sine[angles, :]
        for t in range(tiles):
            qt = turned(q[pl.ds(base, step), t * TILE : (t + 1) * TILE], cos_here, sin_here)
            qt = qt * jnp.bfloat16(HEAD**-0.5)
            zero = jnp.zeros_like(qt)
            q_v[2 * t * step : (2 * t + 1) * step, :] = jnp.where(low, qt, zero)
            q_v[(2 * t + 1) * step : (2 * t + 2) * step, :] = jnp.where(low, zero, qt)
        for g in range(2):
            scores = lax.dot_general(
                q_v[g * heads * step : (g + 1) * heads * step, :],
                k_v[g, pl.ds(base, 3 * WINDOW), :],
                (((1,), (1,)), ((), ())),
                preferred_element_type=jnp.float32,
            )
            exps, denoms = [], []
            for h in range(heads):
                sunk = sink[g * heads + h]
                s = jnp.where(valid, scores[h * step : (h + 1) * step], -jnp.inf)
                top = jnp.maximum(jnp.max(s, 1, keepdims=True), sunk)
                raised = jnp.exp(s - top)
                denoms.append(jnp.sum(raised, 1, keepdims=True) + jnp.exp(sunk - top))
                exps.append(raised.astype(jnp.bfloat16))
            mixed = jnp.dot(
                jnp.concatenate(exps, 0), v_v[g, pl.ds(base, 3 * WINDOW), :],
                preferred_element_type=jnp.float32,
            )
            done = [mixed[h * step : (h + 1) * step] / denoms[h] for h in range(heads)]
            for t in range(2):
                lanes = slice((2 * g + t) * TILE, (2 * g + t + 1) * TILE)
                att_v[pl.ds(to, step), lanes] = jnp.where(low, done[2 * t], done[2 * t + 1]).astype(jnp.bfloat16)
        return 0

    lax.fori_loop(0, 4, one, 0)
    copy.wait()

    def project(n, _):
        at = pl.multiple_of(n * 2 * TILE, 2 * TILE)
        part = jnp.dot(
            att_v[...], weight[:, pl.ds(at, 2 * TILE)], preferred_element_type=jnp.float32
        ).astype(jnp.bfloat16)
        for i, out in enumerate(outs):
            out[:, pl.ds(at, 2 * TILE)] = part[i * share : (i + 1) * share]
        return 0

    lax.fori_loop(0, weight.shape[1] // (2 * TILE), project, 0)


def first_body(
    sink, q, k, v, swapped, across, cosine, sine, weight,
    out1, out3, k_v, v_v, q_v, att_v, cos_v, sin_v, w_v, sem,
):
    copy = pltpu.make_async_copy(weight, w_v, sem)
    copy.start()
    spread_angles(cosine, cos_v, False)
    spread_angles(sine, sin_v, True)
    spread_keys(k, v, swapped, across, cos_v, sin_v, k_v, v_v)
    attend_shares((1, 3), sink, q, cos_v, sin_v, k_v, v_v, copy, w_v, (out1, out3), q_v, att_v)


def second_body(
    sink, q, cosine, sine, k_v, v_v, weight, out2, out0, q_v, att_v, cos_v, sin_v, w_v, sem
):
    copy = pltpu.make_async_copy(weight, w_v, sem)
    copy.start()
    spread_angles(cosine, cos_v, False)
    spread_angles(sine, sin_v, True)
    attend_shares((2, 0), sink, q, cos_v, sin_v, k_v, v_v, copy, w_v, (out2, out0), q_v, att_v)


def attend(sink, q, k, v, swapped, across, cosine, sine, weight):
    rows, width = q.shape
    model = weight.shape[1]
    step = rows // YN // 2
    part = jax.ShapeDtypeStruct((rows // YN, model), jnp.bfloat16)
    spread = jax.ShapeDtypeStruct((2, rows + 3 * WINDOW - step, TILE), jnp.bfloat16)
    scratch = [
        pltpu.VMEM((8 * step, TILE), jnp.bfloat16),
        pltpu.VMEM((rows // 2, width), jnp.bfloat16),
        pltpu.VMEM((rows + 2 * WINDOW, TILE), jnp.float32),
        pltpu.VMEM((rows + 2 * WINDOW, TILE), jnp.float32),
        pltpu.VMEM((width, model), jnp.bfloat16),
        pltpu.SemaphoreType.DMA(()),
    ]
    params = pltpu.CompilerParams(vmem_limit_bytes=32 * 2**20)
    cost = pl.CostEstimate(flops=rows * width * model * 3, bytes_accessed=4 * rows * model, transcendentals=0)
    one, three, keys, values = pl.pallas_call(
        first_body,
        out_shape=(part, part, spread, spread),
        in_specs=[SM] + [VM] * 7 + [HB],
        out_specs=(VM,) * 4,
        scratch_shapes=scratch,
        compiler_params=params,
        cost_estimate=cost,
        name="attend0",
    )(sink, q, k, v, swapped, across, cosine, sine, weight)
    two, zero = pl.pallas_call(
        second_body,
        out_shape=(part, part),
        in_specs=[SM] + [VM] * 5 + [HB],
        out_specs=(VM,) * 2,
        scratch_shapes=scratch,
        compiler_params=params,
        cost_estimate=cost,
        name="attend1",
    )(sink, q, cosine, sine, keys, values, weight)
    return zero, one, two, three


def layer(
    queries, keys, values, sink, stream, out_weight, norm_gain, gate_weight, up_weight, down_weight
):
    sp = lax.axis_index("sp")
    rows = queries.shape[0]
    ends = ZN * XN * CN - 1
    own, theirs, across = packed(gate_weight, up_weight, down_weight, keys, values)
    chips = [(i, i + 1) for i in range(1, ends, CN)]
    across = sp_move(across, chips + [(b, a) for a, b in chips])
    swapped = sp_move(theirs, CORE_SWAP)
    weights = gathered_weights(own, swapped)
    cosine, sine = angle_tables(sp * rows - WINDOW, rows + 2 * WINDOW)
    parts = attend(sink, queries, keys, values, swapped, across, cosine, sine, pltpu.with_memory_space_constraint(out_weight, pltpu.HBM))
    total = stream.astype(jnp.float32) + (
        parts[0].astype(jnp.float32)
        + sum(tp_move(parts[s], s).astype(jnp.float32) for s in (1, 2, 3))
    )
    mixed = total.astype(jnp.bfloat16)
    mixed_wide = mixed.astype(jnp.float32)
    scale = lax.rsqrt(jnp.mean(mixed_wide * mixed_wide, -1, keepdims=True) + 1e-06)
    normed = (mixed_wide * scale * norm_gain).astype(jnp.bfloat16)
    mine = [normed] + [tp_move(normed, s) for s in (1, 2, 3)]
    late = (7, 11, 12, 13)
    early = tuple(i for i in range(len(weights)) if i not in late)
    gu, dt = assembled(weights, late, assembled(weights, early))
    one = jnp.concatenate([lax.optimization_barrier(mine[0]), mine[1]], 0)
    one_there = sp_move(one, CORE_SWAP)
    share = normed.shape[0]
    core = sp_place()[2]
    place = {0: (one, one_there, 0), 1: (one, one_there, share)}
    for s in (2, 3):
        place[s] = (mine[s], sp_move(mine[s], CORE_SWAP), 0)

    def summed(blocks, looped):
        pieces = [(place[s][i], place[s][2]) for i in range(2) for s in blocks]
        kept, sent = ffn(share, pieces, gu, dt, looped)
        return kept.astype(jnp.float32) + sp_move(sent, CORE_SWAP).astype(jnp.float32)

    passed = summed((2,), False).astype(jnp.bfloat16)
    passed = lax.ppermute(passed, ("sp", "tp"), y_apart())
    passed = passed.astype(jnp.float32)
    near = summed((1, 3), True)
    right = near[:share] + jnp.where(core == 0, 0.0, passed)
    right = tp_move(right.astype(jnp.bfloat16), -1)
    left = near[share:] + jnp.where(core == 0, passed, 0.0)
    left = tp_move(left.astype(jnp.bfloat16), 1)
    lowered = summed((0,), True) + right.astype(jnp.float32) + left.astype(jnp.float32)
    return (mixed_wide + 0.5 * lowered).astype(jnp.bfloat16)


def solution(mesh):
    placed = (
        P("sp", "tp"),
        P("sp", "tp"),
        P("sp", "tp"),
        P("tp"),
        P(("sp", "tp"), None),
        P("tp", None),
        P(),
        P("sp", "tp"),
        P("sp", "tp"),
        P("tp", "sp"),
    )
    return jax.shard_map(layer, mesh=mesh, in_specs=placed, out_specs=P(("sp", "tp"), None), check_vma=False)
```

```python
import functools

import jax
import jax.numpy as jnp
from jax import lax
from jax.experimental import pallas as pl
from jax.experimental.pallas import tpu as pltpu
from jax.sharding import PartitionSpec as P


HEAD = 64
WINDOW = 128
ZN, XN, CN, YN = 8, 4, 2, 4
TILE = 128

ANY = pl.BlockSpec(memory_space=pl.ANY)
VM = pl.BlockSpec(memory_space=pltpu.VMEM)
SM = pl.BlockSpec(memory_space=pltpu.SMEM)
HB = pl.BlockSpec(memory_space=pltpu.HBM)


def paired(at, core, step, count):
    turn = core * step if 2 * step < count else 0
    return (((at - turn + count) % count) ^ step) + turn


def z_pairs(step):
    return [
        ((z * XN + x) * CN + c, ((paired(z, c, step, ZN) % ZN) * XN + x) * CN + c)
        for z in range(ZN) for x in range(XN) for c in range(CN)
    ]


def x_shift(s):
    return [
        ((z * XN + x) * CN + c, (z * XN + (x + s) % XN) * CN + c)
        for z in range(ZN) for x in range(XN) for c in range(CN)
    ]


def z_shift(s):
    return [
        ((z * XN + x) * CN + c, (((z + s) % ZN) * XN + x) * CN + c)
        for z in range(ZN) for x in range(XN) for c in range(CN)
    ]


def z_apart():
    return [
        ((z * XN + x) * CN + c, (((z + 1 - 2 * c) % ZN) * XN + x) * CN + c)
        for z in range(ZN) for x in range(XN) for c in range(CN)
    ]


def x_apart():
    return [
        ((z * XN + x) * CN + c, (z * XN + (x + 1 - 2 * c) % XN) * CN + c)
        for z in range(ZN) for x in range(XN) for c in range(CN)
    ]


def y_apart():
    return [
        (((p * CN + c) * YN + y), (p * CN + c) * YN + (y + 1 - 2 * c) % YN)
        for p in range(ZN * XN) for c in range(CN) for y in range(YN)
    ]


CORE_SWAP = [(i, i ^ 1) for i in range(ZN * XN * CN)]


def y_shift(s):
    return [(i, (i + s) % YN) for i in range(YN)]


def sp_move(value, pairs):
    return lax.ppermute(value, "sp", pairs)


def tp_move(value, s):
    return lax.ppermute(value, "tp", y_shift(s))


def pack_body(gate, up, down, k, v, mine, theirs, across):
    full = gate.shape[1] // TILE // CN
    rest = CN * full * TILE
    spare = (gate.shape[1] - rest) // CN
    core = sp_place()[2]

    def put(at, low, high):
        size = low.shape[1]
        mine[:, at : at + size] = jnp.where(core == 0, low, high)
        theirs[:, at : at + size] = jnp.where(core == 0, high, low)

    at = 0
    for j in range(full):
        for value in (gate, up):
            high = (full + j) * TILE
            put(at, value[:, j * TILE : (j + 1) * TILE], value[:, high : high + TILE])
            at += TILE
    last = [value[:, rest:].astype(jnp.float32) for value in (gate, up, down)]
    other = [pltpu.roll(value, TILE // 2, 1) for value in last]
    low = lax.broadcasted_iota(jnp.int32, last[0].shape, 1) < spare
    narrow = jnp.bfloat16
    put(at, jnp.where(low, last[0], other[1]).astype(narrow), jnp.where(low, other[0], last[1]).astype(narrow))
    at += TILE
    for j in range(full):
        high = (full + j) * TILE
        put(at, down[:, j * TILE : (j + 1) * TILE], down[:, high : high + TILE])
        at += TILE
    put(at, jnp.where(low, last[2], 0.0).astype(narrow), jnp.where(low, other[2], 0.0).astype(narrow))
    at += TILE
    depth = gate.shape[0]
    for lane, value in enumerate((k, v)):
        tail, head = value[value.shape[0] - WINDOW :, :], value[:WINDOW, :]
        across[:, lane * TILE : (lane + 1) * TILE] = jnp.where(core == 0, head, tail)
        kept = jnp.where(core == 0, tail, head)
        for i in range(WINDOW // depth):
            lanes = slice(at + (2 * i + lane) * TILE, at + (2 * i + lane + 1) * TILE)
            theirs[:, lanes] = kept[i * depth : (i + 1) * depth]


def packed(gate, up, down, k, v):
    depth, wide = gate.shape[0], 11 * TILE + 6 * TILE
    shard = jax.ShapeDtypeStruct((depth, wide), gate.dtype)
    wider = jax.ShapeDtypeStruct((depth, wide + WINDOW // depth * 2 * TILE), gate.dtype)
    halo = jax.ShapeDtypeStruct((WINDOW, 2 * TILE), k.dtype)
    return pl.pallas_call(
        pack_body,
        out_shape=(shard, wider, halo),
        in_specs=[VM] * 5,
        out_specs=(VM,) * 3,
        name="pack",
    )(gate, up, down.T, k, v)


def gathered_weights(mine, swapped):
    def met(value, pairs):
        return jnp.concatenate([value, sp_move(value, pairs)], 0)

    first = jnp.concatenate([mine] + [sp_move(mine, x_shift(i)) for i in (1, 2, 3)], 0)
    right, left, ups, downs = first, first, [], []
    for _ in range(3):
        right = sp_move(right, z_shift(1))
        left = sp_move(left, z_shift(-1))
        ups.append(right)
        downs.append(left)
    opposite = jnp.where(sp_place()[2] == 0, right, left)
    apart = sp_move(opposite, z_apart())
    near = met(met(swapped[:, : mine.shape[1]], z_pairs(4)), z_pairs(2))
    far = sp_move(near, z_pairs(1))
    nears = [near] + [sp_move(near, x_shift(i)) for i in (1, 3)]
    nears.append(sp_move(jnp.where(sp_place()[2] == 0, *nears[1:]), x_apart()))
    fars = [far] + [sp_move(far, x_shift(i)) for i in (1, 3)]
    fars.append(sp_move(jnp.where(sp_place()[2] == 0, *fars[1:]), x_apart()))
    return (first, *ups, *downs, apart, *nears, *fars)


def weight_blocks(z, x, c):
    xs = [x + XN - back for back in range(XN)]
    found = []
    for array, back in enumerate((0, 1, 2, 3, -1, -2, -3)):
        found += [(array, i, z + ZN - back, at, c) for i, at in enumerate(xs)]
    found += [(7, i, z + 4, at, c) for i, at in enumerate(xs)]
    array = 8
    for low in (z, paired(z, c, 1, ZN)):
        over = paired(low % ZN, c, 2, ZN)
        zs = (low, low + 4, over, over + 4)
        for at in (xs[0], xs[1], xs[3], xs[2]):
            found += [(array, j, zz, at, 1 - c) for j, zz in enumerate(zs)]
            array += 1
    return found


def sp_place():
    sp = lax.axis_index("sp").astype(jnp.int32)
    return sp // (XN * CN), lax.rem(sp // CN, XN), lax.rem(sp, CN)


def assemble_body(*refs, chosen, started):
    count = len(chosen)
    weights = refs[:count]
    whole, sem = refs[count + (1 if started else 0) :]
    depth = whole.shape[0] // (ZN * XN * CN)
    total = 0
    for array, block, z, x, c in weight_blocks(*sp_place()):
        if array not in chosen:
            continue
        who = (lax.rem(z, ZN) * XN + lax.rem(x, XN)) * CN + c
        spot = pl.ds(pl.multiple_of(who * depth, depth), depth)
        ref = weights[chosen.index(array)]
        pltpu.make_async_copy(ref.at[pl.ds(block * depth, depth)], whole.at[spot], sem).start()
        total += depth
    moved = whole.at[pl.ds(0, total)]
    pltpu.make_async_copy(moved, moved, sem).wait()


def assembled(weights, chosen, begun=()):
    model, wide = weights[0].shape[0] // XN * ZN * XN * CN, weights[0].shape[1]
    count = len(chosen)
    return pl.pallas_call(
        functools.partial(assemble_body, chosen=chosen, started=bool(begun)),
        out_shape=jax.ShapeDtypeStruct((model, wide), jnp.bfloat16),
        in_specs=[ANY] * count + [VM] * len(begun),
        out_specs=VM,
        scratch_shapes=[pltpu.SemaphoreType.DMA(())],
        input_output_aliases={count + i: i for i in range(len(begun))},
        compiler_params=pltpu.CompilerParams(vmem_limit_bytes=16 * 2**20),
        cost_estimate=pl.CostEstimate(flops=10**6, bytes_accessed=2 * model * wide, transcendentals=0),
    )(*(weights[i] for i in chosen), *begun)


def ffn_body(*refs, starts, looped):
    xs, (whole, kept, sent, x_v, h_v, sem) = refs[:-6], refs[-6:]
    gu_width = whole.shape[1] - h_v.shape[1]
    rows = x_v.shape[0] // len(xs)
    copies = [
        pltpu.make_async_copy(ref.at[pl.ds(start, rows)], x_v.at[pl.ds(i * rows, rows)], sem.at[i])
        for i, (ref, start) in enumerate(zip(xs, starts))
    ]
    for copy in copies:
        copy.start()
    for copy in copies:
        copy.wait()
    pairs = gu_width // (2 * TILE)
    some = kept.shape[0]

    def activated(gate, upward):
        return gate / (1.0 + jnp.exp(-gate)) * upward

    if not looped:
        both = jnp.dot(x_v[...], whole[:, :gu_width], preferred_element_type=jnp.float32)
        for j in range(pairs):
            gate, upward = (both[:, i * TILE : (i + 1) * TILE] for i in (2 * j, 2 * j + 1))
            h_v[:, j * TILE : (j + 1) * TILE] = activated(gate, upward).astype(jnp.bfloat16)
        gate = both[:, pairs * 2 * TILE :]
    else:

        def gated(j, _):
            at = pl.multiple_of(j * 2 * TILE, 2 * TILE)
            both = jnp.dot(x_v[...], whole[:, pl.ds(at, 2 * TILE)], preferred_element_type=jnp.float32)
            hidden = activated(both[:, :TILE], both[:, TILE:])
            h_v[:, pl.ds(pl.multiple_of(j * TILE, TILE), TILE)] = hidden.astype(jnp.bfloat16)
            return 0

        lax.fori_loop(0, pairs, gated, 0)
        gate = jnp.dot(x_v[...], whole[:, pairs * 2 * TILE : gu_width], preferred_element_type=jnp.float32)
    hidden = activated(gate, pltpu.roll(gate, TILE // 2, 1))
    lane = lax.broadcasted_iota(jnp.int32, hidden.shape, 1)
    h_v[:, pairs * TILE :] = jnp.where(lane < TILE // 2, hidden, 0.0).astype(jnp.bfloat16)
    width = 4 * TILE

    def lowered(n, _):
        at = pl.multiple_of(n * width, width)
        part = lax.dot_general(
            h_v[...], whole[pl.ds(at, width), gu_width:], (((1,), (1,)), ((), ())), preferred_element_type=jnp.float32
        ).astype(jnp.bfloat16)
        kept[:, pl.ds(at, width)] = part[:some]
        sent[:, pl.ds(at, width)] = part[some:]
        return 0

    lax.fori_loop(0, whole.shape[0] // width, lowered, 0)


def ffn(share, pieces, whole, looped):
    model = pieces[0][0].shape[1]
    rows = share * len(pieces)
    half = jax.ShapeDtypeStruct((rows // 2, model), jnp.bfloat16)
    return pl.pallas_call(
        functools.partial(ffn_body, starts=tuple(start for _, start in pieces), looped=looped),
        out_shape=(half, half),
        in_specs=[ANY] * len(pieces) + [VM],
        out_specs=(VM, VM),
        scratch_shapes=[
            pltpu.VMEM((rows, model), jnp.bfloat16),
            pltpu.VMEM((rows, 6 * TILE), jnp.bfloat16),
            pltpu.SemaphoreType.DMA((len(pieces),)),
        ],
        compiler_params=pltpu.CompilerParams(vmem_limit_bytes=24 * 2**20),
        cost_estimate=pl.CostEstimate(
            flops=2 * rows * model * whole.shape[1], bytes_accessed=4 * rows * model,
            transcendentals=0,
        ),
        name="ffn",
    )(*(array for array, _ in pieces), whole)


def angle_tables(start, length):
    lane = jnp.arange(TILE, dtype=jnp.int32)
    entry = lax.rem(lane, HEAD // 2) * 2
    inverse = 1.0 / 10000.0 ** (entry.astype(jnp.float32) / HEAD)
    rows = length // (TILE // (HEAD // 2))
    places = (lane // (HEAD // 2))[None, :] * rows + jnp.arange(rows, dtype=jnp.int32)[:, None]
    angles = (start + places).astype(jnp.float32) * inverse[None, :]
    return jnp.cos(angles), jnp.sin(angles)


def turned(block, cosine, sine):
    wide = block.astype(jnp.float32)
    lane = lax.broadcasted_iota(jnp.int32, wide.shape, 1)
    swapped = jnp.where(
        lax.rem(lane, HEAD) < HEAD // 2,
        pltpu.roll(wide, TILE - HEAD // 2, 1),
        pltpu.roll(wide, HEAD // 2, 1),
    )
    return (wide * cosine + swapped * sine).astype(jnp.bfloat16)


def spread_angles(packed, full, sign):
    rows = packed.shape[0]
    lane = lax.broadcasted_iota(jnp.int32, packed.shape, 1)
    parts = TILE // (HEAD // 2)
    for j in range(parts):
        kept = jnp.where(lane // (HEAD // 2) == j, packed[...], 0.0)
        kept = kept + pltpu.roll(kept, HEAD // 2, 1)
        kept = kept + pltpu.roll(kept, HEAD, 1)
        if sign:
            kept = jnp.where(lax.rem(lane, HEAD) < HEAD // 2, -kept, kept)
        full[j * rows : (j + 1) * rows, :] = kept


def spread_keys(k, v, swapped, across, cosine, sine, k_v, v_v):
    rows = k.shape[0]
    low = lax.broadcasted_iota(jnp.int32, (WINDOW, TILE), 1) < HEAD

    def both_halves(block, g):
        kept = jnp.where(low if g == 0 else ~low, block.astype(jnp.float32), 0.0)
        return (kept + pltpu.roll(kept, HEAD, 1)).astype(jnp.bfloat16)

    blocks = rows // WINDOW
    core = sp_place()[2]
    parts = WINDOW // swapped.shape[0]
    start = swapped.shape[1] - parts * 2 * TILE
    inside = []
    for lane in range(2):
        spots = [start + (2 * i + lane) * TILE for i in range(parts)]
        inside.append(jnp.concatenate([swapped[:, at : at + TILE] for at in spots], 0))
    outside = [across[:, :TILE], across[:, TILE:]]

    def put(at, kb, vb):
        kb = turned(kb, cosine[at, :], sine[at, :])
        for g in range(2):
            k_v[g, at, :] = both_halves(kb, g)
            v_v[g, at, :] = both_halves(vb, g)

    put(slice(0, WINDOW), *(jnp.where(core == 0, a, b) for a, b in zip(outside, inside)))
    for n in range(blocks):
        at = slice(n * WINDOW, (n + 1) * WINDOW)
        put(slice((n + 1) * WINDOW, (n + 2) * WINDOW), k[at, :], v[at, :])
    ends = slice(rows + WINDOW, rows + 2 * WINDOW)
    put(ends, *(jnp.where(core == 0, b, a) for a, b in zip(outside, inside)))
    spare = k_v.shape[1] - rows - 2 * WINDOW
    for g in range(2):
        k_v[g, rows + 2 * WINDOW :, :] = jnp.zeros((spare, TILE), jnp.bfloat16)
        v_v[g, rows + 2 * WINDOW :, :] = jnp.zeros((spare, TILE), jnp.bfloat16)


def attend_shares(shares, sink, q, cosine, sine, k_v, v_v, copy, weight, outs, q_v, att_v):
    rows = q.shape[0]
    share = rows // YN
    step = share // 2
    tiles = q.shape[1] // TILE
    heads = 4
    sp, tp = lax.axis_index("sp").astype(jnp.int32), lax.axis_index("tp").astype(jnp.int32)
    floor = jnp.where(sp == 0, WINDOW, 0)
    ceiling = jnp.where(sp == ZN * XN * CN - 1, rows + WINDOW, rows + 2 * WINDOW)
    low = lax.broadcasted_iota(jnp.int32, (step, TILE), 1) < HEAD
    row = lax.broadcasted_iota(jnp.int32, (step, 3 * WINDOW), 0)
    col = lax.broadcasted_iota(jnp.int32, (step, 3 * WINDOW), 1)
    band = (col >= row) & (col - row <= 2 * WINDOW)

    def one(i, _):
        ahead = jnp.where(i < 2, shares[0], shares[1])
        base = pl.multiple_of(lax.rem(tp + ahead, YN) * share + lax.rem(i, 2) * step, 16)
        to = pl.multiple_of(i * step, 16)
        valid = band & (col >= floor - base) & (col < ceiling - base)
        angles = pl.ds(pl.multiple_of(base + WINDOW, 16), step)
        cos_here, sin_here = cosine[angles, :], sine[angles, :]
        for t in range(tiles):
            qt = turned(q[pl.ds(base, step), t * TILE : (t + 1) * TILE], cos_here, sin_here)
            qt = qt * jnp.bfloat16(HEAD**-0.5)
            zero = jnp.zeros_like(qt)
            q_v[2 * t * step : (2 * t + 1) * step, :] = jnp.where(low, qt, zero)
            q_v[(2 * t + 1) * step : (2 * t + 2) * step, :] = jnp.where(low, zero, qt)
        for g in range(2):
            scores = lax.dot_general(
                q_v[g * heads * step : (g + 1) * heads * step, :],
                k_v[g, pl.ds(base, 3 * WINDOW), :],
                (((1,), (1,)), ((), ())),
                preferred_element_type=jnp.float32,
            )
            exps, denoms = [], []
            for h in range(heads):
                sunk = sink[g * heads + h]
                s = jnp.where(valid, scores[h * step : (h + 1) * step], -jnp.inf)
                top = jnp.maximum(jnp.max(s, 1, keepdims=True), sunk)
                raised = jnp.exp(s - top)
                denoms.append(jnp.sum(raised, 1, keepdims=True) + jnp.exp(sunk - top))
                exps.append(raised.astype(jnp.bfloat16))
            mixed = jnp.dot(
                jnp.concatenate(exps, 0), v_v[g, pl.ds(base, 3 * WINDOW), :],
                preferred_element_type=jnp.float32,
            )
            done = [mixed[h * step : (h + 1) * step] / denoms[h] for h in range(heads)]
            for t in range(2):
                lanes = slice((2 * g + t) * TILE, (2 * g + t + 1) * TILE)
                att_v[pl.ds(to, step), lanes] = jnp.where(low, done[2 * t], done[2 * t + 1]).astype(jnp.bfloat16)
        return 0

    lax.fori_loop(0, 4, one, 0)
    copy.wait()

    def project(n, _):
        at = pl.multiple_of(n * 2 * TILE, 2 * TILE)
        part = jnp.dot(
            att_v[...], weight[:, pl.ds(at, 2 * TILE)], preferred_element_type=jnp.float32
        ).astype(jnp.bfloat16)
        for i, out in enumerate(outs):
            out[:, pl.ds(at, 2 * TILE)] = part[i * share : (i + 1) * share]
        return 0

    lax.fori_loop(0, weight.shape[1] // (2 * TILE), project, 0)


def first_body(
    sink, q, k, v, swapped, across, cosine, sine, weight,
    out1, out3, k_v, v_v, q_v, att_v, cos_v, sin_v, w_v, sem,
):
    copy = pltpu.make_async_copy(weight, w_v, sem)
    copy.start()
    spread_angles(cosine, cos_v, False)
    spread_angles(sine, sin_v, True)
    spread_keys(k, v, swapped, across, cos_v, sin_v, k_v, v_v)
    attend_shares((1, 3), sink, q, cos_v, sin_v, k_v, v_v, copy, w_v, (out1, out3), q_v, att_v)


def second_body(
    sink, q, cosine, sine, k_v, v_v, weight, out2, out0, q_v, att_v, cos_v, sin_v, w_v, sem
):
    copy = pltpu.make_async_copy(weight, w_v, sem)
    copy.start()
    spread_angles(cosine, cos_v, False)
    spread_angles(sine, sin_v, True)
    attend_shares((2, 0), sink, q, cos_v, sin_v, k_v, v_v, copy, w_v, (out2, out0), q_v, att_v)


def attend(sink, q, k, v, swapped, across, cosine, sine, weight):
    rows, width = q.shape
    model = weight.shape[1]
    step = rows // YN // 2
    part = jax.ShapeDtypeStruct((rows // YN, model), jnp.bfloat16)
    spread = jax.ShapeDtypeStruct((2, rows + 3 * WINDOW - step, TILE), jnp.bfloat16)
    scratch = [
        pltpu.VMEM((8 * step, TILE), jnp.bfloat16),
        pltpu.VMEM((rows // 2, width), jnp.bfloat16),
        pltpu.VMEM((rows + 2 * WINDOW, TILE), jnp.float32),
        pltpu.VMEM((rows + 2 * WINDOW, TILE), jnp.float32),
        pltpu.VMEM((width, model), jnp.bfloat16),
        pltpu.SemaphoreType.DMA(()),
    ]
    params = pltpu.CompilerParams(vmem_limit_bytes=32 * 2**20)
    cost = pl.CostEstimate(flops=rows * width * model * 3, bytes_accessed=4 * rows * model, transcendentals=0)
    one, three, keys, values = pl.pallas_call(
        first_body,
        out_shape=(part, part, spread, spread),
        in_specs=[SM] + [VM] * 7 + [HB],
        out_specs=(VM,) * 4,
        scratch_shapes=scratch,
        compiler_params=params,
        cost_estimate=cost,
        name="attend0",
    )(sink, q, k, v, swapped, across, cosine, sine, weight)
    two, zero = pl.pallas_call(
        second_body,
        out_shape=(part, part),
        in_specs=[SM] + [VM] * 5 + [HB],
        out_specs=(VM,) * 2,
        scratch_shapes=scratch,
        compiler_params=params,
        cost_estimate=cost,
        name="attend1",
    )(sink, q, cosine, sine, keys, values, weight)
    return zero, one, two, three


def layer(
    queries, keys, values, sink, stream, out_weight, norm_gain, gate_weight, up_weight, down_weight
):
    sp = lax.axis_index("sp")
    rows = queries.shape[0]
    ends = ZN * XN * CN - 1
    own, theirs, across = packed(gate_weight, up_weight, down_weight, keys, values)
    chips = [(i, i + 1) for i in range(1, ends, CN)]
    across = sp_move(across, chips + [(b, a) for a, b in chips])
    swapped = sp_move(theirs, CORE_SWAP)
    weights = gathered_weights(own, swapped)
    cosine, sine = angle_tables(sp * rows - WINDOW, rows + 2 * WINDOW)
    parts = attend(sink, queries, keys, values, swapped, across, cosine, sine, pltpu.with_memory_space_constraint(out_weight, pltpu.HBM))
    total = stream.astype(jnp.float32) + (
        parts[0].astype(jnp.float32)
        + sum(tp_move(parts[s], s).astype(jnp.float32) for s in (1, 2, 3))
    )
    mixed = total.astype(jnp.bfloat16)
    mixed_wide = mixed.astype(jnp.float32)
    scale = lax.rsqrt(jnp.mean(mixed_wide * mixed_wide, -1, keepdims=True) + 1e-06)
    normed = (mixed_wide * scale * norm_gain).astype(jnp.bfloat16)
    mine = [normed] + [tp_move(normed, s) for s in (1, 2, 3)]
    late = (7, 13, 14, 15)
    early = tuple(i for i in range(len(weights)) if i not in late)
    whole = assembled(weights, late, (assembled(weights, early),))
    one = jnp.concatenate([lax.optimization_barrier(mine[0]), mine[1]], 0)
    one_there = sp_move(one, CORE_SWAP)
    share = normed.shape[0]
    core = sp_place()[2]
    place = {0: (one, one_there, 0), 1: (one, one_there, share)}
    for s in (2, 3):
        place[s] = (mine[s], sp_move(mine[s], CORE_SWAP), 0)

    def summed(blocks, looped):
        pieces = [(place[s][i], place[s][2]) for i in range(2) for s in blocks]
        kept, sent = ffn(share, pieces, whole, looped)
        return kept.astype(jnp.float32) + sp_move(sent, CORE_SWAP).astype(jnp.float32)

    passed = summed((2,), False).astype(jnp.bfloat16)
    passed = lax.ppermute(passed, ("sp", "tp"), y_apart())
    passed = passed.astype(jnp.float32)
    near = summed((1, 3), True)
    right = near[:share] + jnp.where(core == 0, 0.0, passed)
    right = tp_move(right.astype(jnp.bfloat16), -1)
    left = near[share:] + jnp.where(core == 0, passed, 0.0)
    left = tp_move(left.astype(jnp.bfloat16), 1)
    lowered = summed((0,), True) + right.astype(jnp.float32) + left.astype(jnp.float32)
    return (mixed_wide + 0.5 * lowered).astype(jnp.bfloat16)


def solution(mesh):
    placed = (
        P("sp", "tp"),
        P("sp", "tp"),
        P("sp", "tp"),
        P("tp"),
        P(("sp", "tp"), None),
        P("tp", None),
        P(),
        P("sp", "tp"),
        P("sp", "tp"),
        P("tp", "sp"),
    )
    return jax.shard_map(layer, mesh=mesh, in_specs=placed, out_specs=P(("sp", "tp"), None), check_vma=False)
```
